256 devices in a mesh: gr: 2 (over z_hi), fs: 16 (over z_lo, y), tp: 8 (over x, core).
Axes of the slice: x: 4, y: 4, z: 8 (z_hi: 2, z_lo: 4; z = z_hi * 4 + z_lo), core: 2. Of those that a mesh axis runs over, the one named last changes fastest.
Arguments:
- tokens: bfloat16 [8192, 2048], P(('gr', 'fs')), may hold values from -6 to 6
- route_ids: int32 [8192, 4], P(('gr', 'fs')), may hold values from 0 to 15, all different within a row; in each aligned block of 256 rows (0 to 255, 256 to 511, ...) at most 80 rows name the same one
- route_scores: float32 [8192, 4], P(('gr', 'fs')), may hold values from -4 to 4
- norm_gain: float32 [2048], P(('gr', 'fs')), may hold values from 0.1 to 1.9
- gate_weight: float32 [16, 2048, 2048], P(None, ('gr', 'fs'), 'tp'), may hold values from -0.5 to 0.5
- up_weight: float32 [16, 2048, 2048], P(None, ('gr', 'fs'), 'tp'), may hold values from -0.5 to 0.5
- down_weight: float32 [16, 2048, 2048], P(None, ('gr', 'fs'), 'tp'), may hold values from -0.03125 to 0.03125
Outputs:
- served_gate: bfloat16 [16, 2048, 2048], P('fs', None, 'tp')
- served_up: bfloat16 [16, 2048, 2048], P('fs', None, 'tp')
- served_down: bfloat16 [16, 2048, 2048], P('fs', None, 'tp')
- expert_mix: bfloat16 [8192, 2048], P(('gr', 'fs'), 'tp')
The draws below stay inside these ranges and needn't reach their ends.
Inputs may be any that keep to these rules, and one draw needn't show every extreme that they name: `route_ids`: in each aligned block of 256 rows no expert is named by more than 80 pairs, and in some blocks one expert is named by exactly 80. The 4 experts of a token differ.
All inputs are finite; a program needn't handle non-finite values.
Results may differ from the reference program's by a relative error of at most 0.0092.
Values may be sent and summed in bfloat16 or wider, within the bound.
A program may use at most 64 MiB of HBM per device.

```python
import math
import jax
import jax.numpy as jnp
import numpy as np
from jax import lax

D = 2048
FF = 2048
EXPERTS = 16
TOP = 4
TOK_DEV = 256
CAP = 80
TOKENS = 8192


def shard_levels(own_key, dims, cuts, smallest, top_value):
    def one(dim, shards_of):
        draws = jax.random.uniform(jax.random.fold_in(jax.random.fold_in(own_key, 6), dim), (shards_of,), jnp.float32, smallest / len(cuts), top_value / len(cuts))
        return jnp.repeat(jnp.exp(draws), dims[dim] // shards_of).reshape((-1,) + (1,) * (len(dims) - dim - 1))

    factor_of = one(*cuts[0])
    for cut in cuts[1:]:
        factor_of = factor_of * one(*cut)
    return factor_of


def routed_block(stream_key, own, number, rows, number_of, top, reach, lean):
    sequence = jax.random.permutation(stream_key, number_of)
    packed, ordinary = load_shares(number_of, rows * top, reach, lean, True), load_shares(number_of, rows * top, reach, lean, False)
    places = jnp.arange(number_of)

    def named(sizes, turn):
        used = int((sizes > 0).sum())
        fixed = max(1, used // 4)
        moved = fixed + (places - fixed + turn * (used - fixed)) % max(1, number_of - fixed)
        return jnp.zeros((number_of,), jnp.int32).at[sequence[jnp.where(places < fixed, places, moved)]].set(jnp.asarray(sizes, jnp.int32))

    sizes = jnp.where(number % 4 == 0, named(packed, number // 4), named(ordinary, number - number // 4 - 1))
    mixed = jax.random.permutation(jax.random.fold_in(own, 3), number_of)
    donor, receiver = mixed[0:number_of // 2 * 2:2], mixed[1:number_of // 2 * 2:2]
    slack = jnp.minimum(sizes[donor] - 1, reach - sizes[receiver]) // 2
    slack = jnp.where((donor == sequence[0]) | (receiver == sequence[0]) | (sizes[receiver] == 0), 0, jnp.maximum(slack, 0))
    moved = jax.random.randint(jax.random.fold_in(own, 4), (number_of // 2,), 0, 1 << 20) % (slack + 1)
    sizes = sizes.at[donor].add(-moved).at[receiver].add(moved)
    members = jnp.searchsorted(jnp.cumsum(sizes), jnp.arange(rows * top), side="right").astype(jnp.int32)
    table = members.reshape(top, rows).T
    table = table[jax.random.permutation(jax.random.fold_in(own, 1), rows)]
    turn = jax.random.randint(jax.random.fold_in(own, 2), (rows, 1), 0, top)
    return jnp.take_along_axis(table, (jnp.arange(top)[None, :] + turn) % top, axis=1)


def load_shares(amount, total, most, lean, full):
    weights = [(1 << 20) // math.isqrt(grade ** lean) + 1 for grade in range(1, amount + 1)]
    largest = most if full else min(most, max(-(-total // amount), total * weights[0] // sum(weights)))
    least = 1 if total - largest >= amount - 1 else 0
    counts, spare = [largest] + [least] * (amount - 1), total - largest - least * (amount - 1)
    while spare > 0:
        candidates = [i for i in range(1, amount) if counts[i] < largest] or [i for i in range(1, amount) if counts[i] < most]
        pool, left = sum([weights[i] for i in candidates]), spare
        for i in candidates:
            more = min(most - counts[i], max(1, left * weights[i] // pool), spare)
            counts[i] = counts[i] + more
            spare = spare - more
    return np.array(counts)


def bell_draw(stream_key, extent, deviation, limit, split=(), kind=jnp.bfloat16):
    result = jax.random.normal(stream_key, extent, jnp.float32) * deviation
    if len(split) > 0:
        result = shard_levels(stream_key, extent, split, -0.22, 0.18) * result
    return jnp.clip(result, min=-limit, max=limit).astype(kind)


def setup_inputs(seed: int = 0) -> dict:
    splits = jax.random.split(jax.random.key(seed), 8)
    tokens = bell_draw(splits[0], (TOKENS, D), 1.0, 6.0, ((0, 32),))
    route_ids_keys = jax.random.split(jax.random.fold_in(splits[1], 1), TOKENS // TOK_DEV)
    route_ids_turns = jax.random.permutation(jax.random.fold_in(splits[1], 3), TOKENS // TOK_DEV)
    route_ids = jax.vmap(lambda own, number: routed_block(jax.random.fold_in(splits[1], 2), own, number, TOK_DEV, EXPERTS, TOP, CAP, 2))(route_ids_keys, route_ids_turns).reshape((TOKENS, TOP))
    route_scores = bell_draw(splits[2], (TOKENS, TOP), 1.0, 4.0, ((0, 32),), jnp.float32)
    norm_gain = jnp.clip(1.0 + 0.18 * jax.random.normal(splits[3], (D,), jnp.float32), 0.1, 1.9)
    gate_weight = bell_draw(splits[4], (EXPERTS, D, FF), (D // 16) ** -0.5, 0.5, ((1, 32), (2, 8)), jnp.float32)
    up_weight = bell_draw(splits[5], (EXPERTS, D, FF), (D // 16) ** -0.5, 0.5, ((1, 32), (2, 8)), jnp.float32)
    down_weight = bell_draw(splits[6], (EXPERTS, FF, D), (FF * 16) ** -0.5, 0.03125, ((1, 32), (2, 8)), jnp.float32)
    return {"tokens": tokens, "route_ids": route_ids, "route_scores": route_scores, "norm_gain": norm_gain, "gate_weight": gate_weight, "up_weight": up_weight, "down_weight": down_weight}


norm_eps = 1e-06
clamp_limit = 7.0
sigmoid_slope = 1.702

def route_tables(block_ids, block_scores):
    row_count, top_count = block_ids.shape
    flattened = block_ids.reshape(-1)
    onehot = (flattened[:, None] == jnp.arange(EXPERTS, dtype=jnp.int32)[None, :]).astype(jnp.int32)
    before = jnp.cumsum(onehot, axis=0) - onehot
    slot_index = lax.optimization_barrier(jnp.sum(before * onehot, axis=1))
    target = flattened * CAP + slot_index
    matches = (target[:, None] == jnp.arange(EXPERTS * CAP, dtype=jnp.int32)[None, :]).astype(jnp.float32)
    matches = matches.reshape(row_count, top_count, EXPERTS * CAP)
    exponent = jnp.exp(block_scores.astype(jnp.float32))
    weights = (exponent / lax.optimization_barrier(jnp.sum(exponent, axis=1, keepdims=True))).astype(jnp.bfloat16)
    dispatch = lax.optimization_barrier(jnp.sum(matches, axis=1)).T.astype(jnp.bfloat16)
    combine = jnp.einsum('tk,tkc->tc', weights.astype(jnp.float32), matches).astype(jnp.bfloat16)
    return (dispatch, combine)

def activate(gate_pre, up_pre):
    clipped_gate = jnp.minimum(gate_pre, clamp_limit)
    clipped_up = jnp.clip(up_pre, -clamp_limit, clamp_limit)
    return (clipped_gate * jax.nn.sigmoid(sigmoid_slope * clipped_gate) * (clipped_up + 1.0)).astype(jnp.bfloat16)

def reference(tokens, route_ids, route_scores, norm_gain, gate_weight, up_weight, down_weight):
    served_gate = (norm_gain[None, :, None] * gate_weight).astype(jnp.bfloat16)
    served_up = (norm_gain[None, :, None] * up_weight).astype(jnp.bfloat16)
    served_down = down_weight.astype(jnp.bfloat16)
    as_float = tokens.astype(jnp.float32)
    normed = (as_float * lax.rsqrt(lax.optimization_barrier(jnp.mean(as_float * as_float, axis=1, keepdims=True)) + norm_eps)).astype(jnp.bfloat16)
    blocks = tokens.shape[0] // TOK_DEV
    block_ids = route_ids.reshape(blocks, TOK_DEV, TOP)
    block_scores = route_scores.reshape(blocks, TOK_DEV, TOP)
    block_rows = normed.reshape(blocks, TOK_DEV, D)

    def build(inputs):
        dispatch, combine = route_tables(inputs[0], inputs[1])
        filled = jnp.dot(dispatch, inputs[2], preferred_element_type=jnp.float32).astype(jnp.bfloat16)
        return (filled, combine)
    slot_rows, combines = lax.map(build, (block_ids, block_scores, block_rows))
    by_expert = slot_rows.reshape(blocks, EXPERTS, CAP, D).transpose(1, 0, 2, 3).reshape(EXPERTS, blocks * CAP, D)

    def expert(inputs):
        arrived, gate_mat, up_mat, down_mat = inputs
        gate_pre = jnp.dot(arrived, gate_mat, preferred_element_type=jnp.float32)
        up_pre = jnp.dot(arrived, up_mat, preferred_element_type=jnp.float32)
        hidden = activate(gate_pre, up_pre)
        return jnp.dot(hidden, down_mat, preferred_element_type=jnp.float32).astype(jnp.bfloat16)
    slot_out = lax.map(expert, (by_expert, served_gate, served_up, served_down))
    returned = slot_out.reshape(EXPERTS, blocks, CAP, D).transpose(1, 0, 2, 3).reshape(blocks, EXPERTS * CAP, D)

    def mix(inputs):
        return jnp.dot(inputs[0], inputs[1], preferred_element_type=jnp.float32).astype(jnp.bfloat16)
    expert_mix = lax.map(mix, (combines, returned)).reshape(blocks * TOK_DEV, D)
    return (served_gate, served_up, served_down, expert_mix)
```

```python
import jax
import jax.numpy as jnp
from jax import lax
from jax.experimental import pallas as pl
from jax.experimental.pallas import tpu as pltpu
from jax.sharding import PartitionSpec as P

MESH = pl.DeviceIdType.MESH
BF16, F32 = jnp.bfloat16, jnp.float32

EXPERTS = 16
TOP = 4
CAP = 80
ROWS = 256
SLOTS = EXPERTS * CAP
COLS = 256
TPS = 8
ZS, YS, XS = 8, 4, 4
OWN = 64
CHUNKS = 4
CHUNK = SLOTS // CHUNKS
HALF = CHUNK // 2

norm_eps = 1e-06
clamp_limit = 7.0
sigmoid_slope = 1.702


def rem(a, n):
    return lax.rem(a, n)


def kernel(
    tok_h, ids_h, sc_h, gain_h, gate_h, up_h, down_h,
    og, ou, od, om,
    tok_v, ids_v, sc_v, gain_v, gate_v, up_v, down_v,
    qt, wt, onehot, combine_t, normed, slots,
    wb1, wb2, rcv1, rcv2, ag1, ag2, acc, res, ret, mix_v,
    load_sem, out_sem, tok_send, tok_recv, w1_send, w2_send, w1_recv, w2_recv,
    ag1_send, ag2_send, ag1_recv, ag2_recv, ret_send, ret_recv,
):
    gr, fs, tp = lax.axis_index("gr"), lax.axis_index("fs"), lax.axis_index("tp")
    z, y = gr * 4 + fs // 4, rem(fs, 4)
    x, core = tp // 2, rem(tp, 2)
    me = z * YS + y

    def at(zz, yy):
        return (zz // 4, rem(zz, 4) * 4 + yy, tp)

    def along(xx, cc):
        return (gr, fs, xx * 2 + cc)

    x_right, x_left, x_far = rem(x + 1, XS), rem(x + 3, XS), rem(x + 2, XS)
    right, left, sib = along(x_right, core), along(x_left, core), along(x, 1 - core)

    def remote(src, dst, send, recv, device):
        return pltpu.make_async_remote_copy(
            src_ref=src, dst_ref=dst, send_sem=send, recv_sem=recv,
            device_id=device, device_id_type=MESH,
        )

    def landed(ref, sem):
        pltpu.make_async_copy(ref, ref, sem).wait()

    loads = [
        pltpu.make_async_copy(s, d, load_sem.at[i])
        for i, (s, d) in enumerate(
            ((ids_h, ids_v), (sc_h, sc_v), (tok_h, tok_v), (gain_h, gain_v),
             (gate_h, gate_v), (up_h, up_v), (down_h, down_v))
        )
    ]
    for c in loads:
        c.start()

    barrier = pltpu.get_barrier_semaphore()

    def greet(i, carry):
        zz, yy = rem(z + i // 4, ZS), rem(y + rem(i, 4), YS)
        pl.semaphore_signal(barrier, inc=1, device_id=at(zz, yy), device_id_type=MESH)
        return carry

    lax.fori_loop(1, ZS * YS, greet, 0)
    for d in (right, left, sib):
        pl.semaphore_signal(barrier, inc=1, device_id=d, device_id_type=MESH)

    loads[0].wait()
    loads[1].wait()
    ids = ids_v[...]
    exponent = jnp.exp(sc_v[...])
    total = jnp.sum(exponent, axis=0, keepdims=True)
    weights = (exponent / total).astype(BF16).astype(F32)
    expert_of = lax.broadcasted_iota(jnp.int32, (EXPERTS, ROWS), 0)
    member = jnp.zeros((EXPERTS, ROWS), F32)
    weight_of = jnp.zeros((EXPERTS, ROWS), F32)
    for k in range(TOP):
        same = ids[k : k + 1, :] == expert_of
        member = member + jnp.where(same, 1.0, 0.0)
        weight_of = weight_of + jnp.where(same, weights[k : k + 1, :], 0.0)
    earlier = jnp.where(
        lax.broadcasted_iota(jnp.int32, (ROWS, ROWS), 0)
        < lax.broadcasted_iota(jnp.int32, (ROWS, ROWS), 1),
        1.0, 0.0,
    ).astype(BF16)
    before = jnp.dot(member.astype(BF16), earlier, preferred_element_type=F32)
    qt[...] = jnp.where(member > 0.5, before, -1.0)
    wt[...] = weight_of

    slot_no = lax.broadcasted_iota(jnp.int32, (CAP, ROWS), 0).astype(F32)

    def tables(e, carry):
        hit = qt[pl.ds(e, 1), :] == slot_no
        rows = pl.ds(pl.multiple_of(e * CAP, 16), CAP)
        onehot[rows, :] = jnp.where(hit, 1.0, 0.0).astype(BF16)
        combine_t[rows, :] = jnp.where(hit, wt[pl.ds(e, 1), :], 0.0).astype(BF16)
        return carry

    lax.fori_loop(0, EXPERTS, tables, 0)

    loads[2].wait()

    def norm(i, carry):
        rows = pl.ds(pl.multiple_of(i * 32, 32), 32)
        full = tok_v[rows, :].astype(F32)
        scale = lax.rsqrt(jnp.mean(full * full, axis=1, keepdims=True) + norm_eps)
        mine = tok_v[rows, pl.ds(pl.multiple_of(tp * COLS, COLS), COLS)].astype(F32)
        normed[rows, :] = (mine * scale).astype(BF16)
        return carry

    lax.fori_loop(0, ROWS // 32, norm, 0)

    def fill(i, carry):
        rows = pl.ds(pl.multiple_of(i * CHUNK, CHUNK), CHUNK)
        slots[rows, :] = jnp.dot(
            onehot[rows, :], normed[...], preferred_element_type=F32
        ).astype(BF16)
        return carry

    lax.fori_loop(0, CHUNKS, fill, 0)

    loads[3].wait()
    square = (OWN, OWN)
    gain = jnp.sum(
        jnp.where(
            lax.broadcasted_iota(jnp.int32, square, 0) == lax.broadcasted_iota(jnp.int32, square, 1),
            jnp.broadcast_to(gain_v[...], square), 0.0,
        ),
        axis=1, keepdims=True,
    )
    for i in (4, 5, 6):
        loads[i].wait()

    def fold(e, carry):
        wb1[e, :, 0:COLS] = (gain * gate_v[e]).astype(BF16)
        wb1[e, :, COLS : 2 * COLS] = (gain * up_v[e]).astype(BF16)
        wb2[e] = down_v[e].astype(BF16)
        return carry

    lax.fori_loop(0, EXPERTS, fold, 0)
    own_rows = pl.ds(pl.multiple_of(me * OWN, OWN), OWN)
    rcv1[own_rows, :] = wb1[fs]
    rcv2[own_rows, :] = wb2[fs]

    def slot_rows(e):
        return pl.ds(pl.multiple_of(e * CAP, 16), CAP)

    self_slot = 3 * 4 + y
    ag1[tp, slot_rows(self_slot), :] = slots[slot_rows(fs), :]

    pl.semaphore_wait(barrier, ZS * YS - 1 + 3)

    def send_slots(zt, yt, group):
        e = rem(zt, 4) * 4 + yt
        remote(
            slots.at[slot_rows(e)], ag1.at[tp, slot_rows(group * 4 + y)],
            tok_send, tok_recv, at(zt, yt),
        ).start()

    def two_away(yt, carry):
        step = jnp.where(rem(y + yt, 2) == 0, 2, 6)
        send_slots(rem(z + step, ZS), yt, 0)
        return carry

    lax.fori_loop(0, YS, two_away, 0)

    def one_away(yt, carry):
        send_slots(rem(z + 1, ZS), yt, 1)
        send_slots(rem(z + 7, ZS), yt, 2)
        return carry

    lax.fori_loop(0, YS, one_away, 0)

    def same_plane(i, carry):
        send_slots(z, rem(y + i, YS), 3)
        return carry

    lax.fori_loop(1, YS, same_plane, 0)

    def plane(k):
        away = (k + 1) // 2
        return rem(z + jnp.where(rem(k, 2) == 1, away, ZS - away), ZS)

    def send_weights(source, landing, send, recv):
        def one(i, carry):
            zt, yt = plane(i // 4), rem(y + rem(i, 4), YS)
            remote(
                source.at[rem(zt, 4) * 4 + yt], landing.at[own_rows],
                send, recv.at[z], at(zt, yt),
            ).start()
            return carry

        lax.fori_loop(1, ZS * YS, one, 0)

    send_weights(wb1, rcv1, w1_send, w1_recv)
    send_weights(wb2, rcv2, w2_send, w2_recv)

    def chunk_rows(q):
        return pl.ds(q * CHUNK, CHUNK)

    def gather(buf, send, recv):
        def own(q):
            piece = buf.at[tp, chunk_rows(q)]
            remote(piece, piece, send, recv.at[0, q], right).start()
            remote(piece, piece, send, recv.at[1, q], left).start()
            remote(piece, piece, send, recv.at[4, q], sib).start()

        def forward(q):
            from_left = buf.at[x_left * 2 + core, chunk_rows(q)]
            landed(from_left, recv.at[0, q])
            first = buf.at[x_left * 2 + core, pl.ds(q * CHUNK, HALF)]
            remote(first, first, send, recv.at[2, q], right).start()
            remote(from_left, from_left, send, recv.at[5, q], sib).start()
            from_right = buf.at[x_right * 2 + core, chunk_rows(q)]
            landed(from_right, recv.at[1, q])
            second = buf.at[x_right * 2 + core, pl.ds(q * CHUNK + HALF, HALF)]
            remote(second, second, send, recv.at[3, q], left).start()
            remote(from_right, from_right, send, recv.at[6, q], sib).start()

        def far(q):
            landed(buf.at[x_far * 2 + core, pl.ds(q * CHUNK, HALF)], recv.at[2, q])
            landed(buf.at[x_far * 2 + core, pl.ds(q * CHUNK + HALF, HALF)], recv.at[3, q])
            piece = buf.at[x_far * 2 + core, chunk_rows(q)]
            remote(piece, piece, send, recv.at[7, q], sib).start()

        def others(q):
            for i, xx in ((4, x), (5, x_left), (6, x_right), (7, x_far)):
                landed(buf.at[xx * 2 + 1 - core, chunk_rows(q)], recv.at[i, q])

        return own, forward, far, others

    own, forward, far, others = gather(ag1, ag1_send, ag1_recv)
    landed(ag1.at[0, pl.ds(0, SLOTS - CAP)], tok_recv)
    own(0)
    own(1)
    for q in range(CHUNKS):
        forward(q)
        if q + 2 < CHUNKS:
            own(q + 2)
    for q in range(CHUNKS):
        far(q)
    for q in range(CHUNKS):
        others(q)

    def dot_rows(j, rows):
        return jnp.dot(
            ag1[j, rows, :], rcv1[pl.ds(pl.multiple_of(j * COLS, COLS), COLS), :],
            preferred_element_type=F32,
        )

    def spread(r):
        return pl.ds(pl.multiple_of(r * CHUNK, CHUNK), CHUNK)

    landed(rcv1.at[pl.ds(0, 3 * OWN)], w1_recv.at[z])

    def first_plane(r, carry):
        acc[spread(r), :] = dot_rows(z, spread(r))
        return carry

    lax.fori_loop(0, CHUNKS, first_plane, 0)

    def next_plane(k, carry):
        j = plane(k)
        landed(rcv1.at[pl.ds(0, 4 * OWN)], w1_recv.at[j])

        def more(r, inner):
            acc[spread(r), :] += dot_rows(j, spread(r))
            return inner

        return lax.fori_loop(0, CHUNKS, more, carry)

    lax.fori_loop(1, ZS - 1, next_plane, 0)
    last = plane(ZS - 1)
    landed(rcv1.at[pl.ds(0, 4 * OWN)], w1_recv.at[last])

    own, forward, far, others = gather(ag2, ag2_send, ag2_recv)

    def produce(q):
        rows = chunk_rows(q)
        pre = acc[rows, :] + dot_rows(last, rows)
        g = jnp.minimum(pre[:, :COLS], clamp_limit)
        v = jnp.clip(pre[:, COLS:], -clamp_limit, clamp_limit)
        ag2[tp, rows, :] = (g * jax.nn.sigmoid(sigmoid_slope * g) * (v + 1.0)).astype(BF16)

    produce(0)
    own(0)
    produce(1)
    own(1)
    produce(2)
    produce(3)
    outs = [
        pltpu.make_async_copy(rcv1.at[:, pl.ds(0, COLS)], og.at[0], out_sem.at[0]),
        pltpu.make_async_copy(rcv1.at[:, pl.ds(COLS, COLS)], ou.at[0], out_sem.at[1]),
        pltpu.make_async_copy(rcv2, od.at[0], out_sem.at[2]),
    ]
    outs[0].start()
    outs[1].start()
    for q in range(CHUNKS):
        forward(q)
        if q + 2 < CHUNKS:
            own(q + 2)
    for q in range(CHUNKS):
        far(q)

    landed(rcv2.at[pl.ds(0, 3 * OWN)], w2_recv.at[z])

    def down_landed(k, carry):
        landed(rcv2.at[pl.ds(0, 4 * OWN)], w2_recv.at[plane(k)])
        return carry

    lax.fori_loop(1, ZS, down_landed, 0)
    outs[2].start()

    def finish(q):
        others(q)
        rows = chunk_rows(q)
        summed = jnp.zeros((CHUNK, COLS), F32)
        for j in range(TPS):
            summed = summed + jnp.dot(
                ag2[j, rows, :], rcv2[j * COLS : (j + 1) * COLS, :], preferred_element_type=F32
            )
        res[rows, :] = summed.astype(BF16)

    def send_back(group, ys, zs):
        remote(
            res.at[slot_rows(group * 4 + ys)], ret.at[slot_rows(fs)],
            ret_send, ret_recv, at(zs, ys),
        ).start()

    def back_two(ys, carry):
        step = jnp.where(rem(y + ys, 2) == 0, 6, 2)
        send_back(0, ys, rem(z + step, ZS))
        return carry

    finish(0)
    lax.fori_loop(0, YS, back_two, 0)

    def back_left(ys, carry):
        send_back(1, ys, rem(z + 7, ZS))
        return carry

    finish(1)
    lax.fori_loop(0, YS, back_left, 0)

    def back_right(ys, carry):
        send_back(2, ys, rem(z + 1, ZS))
        return carry

    finish(2)
    lax.fori_loop(0, YS, back_right, 0)

    def back_here(i, carry):
        send_back(3, rem(y + i, YS), z)
        return carry

    finish(3)
    lax.fori_loop(1, YS, back_here, 0)
    ret[slot_rows(fs), :] = res[slot_rows(self_slot), :]

    landed(ret.at[pl.ds(0, SLOTS - CAP)], ret_recv)
    mix_v[...] = lax.dot_general(
        combine_t[...], ret[...], (((0,), (0,)), ((), ())), preferred_element_type=F32
    ).astype(BF16)
    mix_out = pltpu.make_async_copy(mix_v, om, out_sem.at[3])
    mix_out.start()

    landed(slots.at[pl.ds(0, SLOTS - CAP)], tok_send)
    landed(ret.at[pl.ds(0, SLOTS - CAP)], ret_send)
    landed(rcv1.at[pl.ds(0, 31 * OWN)], w1_send)
    landed(rcv2.at[pl.ds(0, 31 * OWN)], w2_send)
    landed(ag1.at[pl.ds(0, 7)], ag1_send)
    landed(ag2.at[pl.ds(0, 7)], ag2_send)
    for c in outs:
        c.wait()
    mix_out.wait()


def local(tokens, route_ids, route_scores, norm_gain, gate_weight, up_weight, down_weight):
    anywhere = pl.BlockSpec(memory_space=pl.ANY)
    dma = pltpu.SemaphoreType.DMA
    served = jax.ShapeDtypeStruct((1, 2048, COLS), BF16)
    return pl.pallas_call(
        kernel,
        name="hand_over",
        out_shape=(served, served, served, jax.ShapeDtypeStruct((ROWS, COLS), BF16)),
        in_specs=[anywhere] * 7,
        out_specs=[anywhere] * 4,
        scratch_shapes=[
            pltpu.VMEM((ROWS, 2048), BF16),
            pltpu.VMEM((TOP, ROWS), jnp.int32),
            pltpu.VMEM((TOP, ROWS), F32),
            pltpu.VMEM((1, OWN), F32),
            pltpu.VMEM((EXPERTS, OWN, COLS), F32),
            pltpu.VMEM((EXPERTS, OWN, COLS), F32),
            pltpu.VMEM((EXPERTS, OWN, COLS), F32),
            pltpu.VMEM((EXPERTS, ROWS), F32),
            pltpu.VMEM((EXPERTS, ROWS), F32),
            pltpu.VMEM((SLOTS, ROWS), BF16),
            pltpu.VMEM((SLOTS, ROWS), BF16),
            pltpu.VMEM((ROWS, COLS), BF16),
            pltpu.VMEM((SLOTS, COLS), BF16),
            pltpu.VMEM((EXPERTS, OWN, 2 * COLS), BF16),
            pltpu.VMEM((EXPERTS, OWN, COLS), BF16),
            pltpu.VMEM((2048, 2 * COLS), BF16),
            pltpu.VMEM((2048, COLS), BF16),
            pltpu.VMEM((TPS, SLOTS, COLS), BF16),
            pltpu.VMEM((TPS, SLOTS, COLS), BF16),
            pltpu.VMEM((SLOTS, 2 * COLS), F32),
            pltpu.VMEM((SLOTS, COLS), BF16),
            pltpu.VMEM((SLOTS, COLS), BF16),
            pltpu.VMEM((ROWS, COLS), BF16),
            dma((7,)), dma((4,)), dma(()), dma(()), dma(()), dma(()), dma((ZS,)), dma((ZS,)),
            dma(()), dma(()), dma((8, CHUNKS)), dma((8, CHUNKS)), dma(()), dma(()),
        ],
        compiler_params=pltpu.CompilerParams(
            collective_id=0, has_side_effects=True, vmem_limit_bytes=56 * 1024 * 1024
        ),
    )(
        tokens, route_ids.T, route_scores.T, norm_gain.reshape(1, OWN),
        gate_weight, up_weight, down_weight,
    )


def solution(mesh):
    in_specs = (
        P(("gr", "fs"), None),
        P(("gr", "fs"), None),
        P(("gr", "fs"), None),
        P(("gr", "fs")),
        P(None, ("gr", "fs"), "tp"),
        P(None, ("gr", "fs"), "tp"),
        P(None, ("gr", "fs"), "tp"),
    )
    out_specs = (
        P("fs", None, "tp"),
        P("fs", None, "tp"),
        P("fs", None, "tp"),
        P(("gr", "fs"), "tp"),
    )
    return jax.shard_map(local, mesh=mesh, in_specs=in_specs, out_specs=out_specs, check_vma=False)
```

```python
import jax
import jax.numpy as jnp
from jax import lax
from jax.experimental import pallas as pl
from jax.experimental.pallas import tpu as pltpu
from jax.sharding import PartitionSpec as P

MESH = pl.DeviceIdType.MESH
BF16, F32 = jnp.bfloat16, jnp.float32

EXPERTS = 16
TOP = 4
CAP = 80
ROWS = 256
SLOTS = EXPERTS * CAP
COLS = 256
SIDE = COLS // 2
TPS = 8
ZS, YS, XS = 8, 4, 4
OWN = 64
CHUNKS = 4
CHUNK = SLOTS // CHUNKS
HALF = CHUNK // 2
EARLY = 5

norm_eps = 1e-06
clamp_limit = 7.0
sigmoid_slope = 1.702


def rem(a, n):
    return lax.rem(a, n)


def kernel(
    tok_h, ids_h, sc_h, gain_h, gate_h, up_h, down_h,
    rcv1a, rcv1b, rcv2, ret, combine_t,
    tok_v, ids_v, sc_v, gain_v, gate_v, up_v, down_v,
    qt, wt, onehot, normed, slots,
    wb1a, wb1b, wb2, ag1, ag2, acc, res,
    load_sem, tok_send, tok_recv, w_send, w1a_recv, w1b_recv, w2_recv,
    ag_send, ag1_recv, ag2a_recv, ag2b_recv, ret_send, ret_recv,
):
    gr, fs, tp = lax.axis_index("gr"), lax.axis_index("fs"), lax.axis_index("tp")
    z, y = gr * 4 + fs // 4, rem(fs, 4)
    x, core = tp // 2, rem(tp, 2)
    me = z * YS + y

    def at(zz, yy):
        return (zz // 4, rem(zz, 4) * 4 + yy, tp)

    def along(xx, cc):
        return (gr, fs, xx * 2 + cc)

    x_right, x_left, x_far = rem(x + 1, XS), rem(x + 3, XS), rem(x + 2, XS)
    right, left, sib = along(x_right, core), along(x_left, core), along(x, 1 - core)

    def remote(src, dst, send, recv, device):
        return pltpu.make_async_remote_copy(
            src_ref=src, dst_ref=dst, send_sem=send, recv_sem=recv,
            device_id=device, device_id_type=MESH,
        )

    def landed(ref, sem):
        pltpu.make_async_copy(ref, ref, sem).wait()

    loads = [
        pltpu.make_async_copy(s, d, load_sem.at[i])
        for i, (s, d) in enumerate(
            ((ids_h, ids_v), (sc_h, sc_v), (tok_h, tok_v), (gain_h, gain_v),
             (gate_h, gate_v), (up_h, up_v), (down_h, down_v))
        )
    ]
    for c in loads:
        c.start()

    barrier = pltpu.get_barrier_semaphore()

    def greet(i, carry):
        zz, yy = rem(z + i // 4, ZS), rem(y + rem(i, 4), YS)
        pl.semaphore_signal(barrier, inc=1, device_id=at(zz, yy), device_id_type=MESH)
        return carry

    lax.fori_loop(1, ZS * YS, greet, 0)
    for d in (right, left, sib):
        pl.semaphore_signal(barrier, inc=1, device_id=d, device_id_type=MESH)

    loads[0].wait()
    loads[1].wait()
    ids = ids_v[...]
    exponent = jnp.exp(sc_v[...])
    total = jnp.sum(exponent, axis=0, keepdims=True)
    weights = (exponent / total).astype(BF16).astype(F32)
    expert_of = lax.broadcasted_iota(jnp.int32, (EXPERTS, ROWS), 0)
    member = jnp.zeros((EXPERTS, ROWS), F32)
    weight_of = jnp.zeros((EXPERTS, ROWS), F32)
    for k in range(TOP):
        same = ids[k : k + 1, :] == expert_of
        member = member + jnp.where(same, 1.0, 0.0)
        weight_of = weight_of + jnp.where(same, weights[k : k + 1, :], 0.0)
    earlier = jnp.where(
        lax.broadcasted_iota(jnp.int32, (ROWS, ROWS), 0)
        < lax.broadcasted_iota(jnp.int32, (ROWS, ROWS), 1),
        1.0, 0.0,
    ).astype(BF16)
    before = jnp.dot(member.astype(BF16), earlier, preferred_element_type=F32)
    qt[...] = jnp.where(member > 0.5, before, -1.0)
    wt[...] = weight_of

    slot_no = lax.broadcasted_iota(jnp.int32, (CAP, ROWS), 0).astype(F32)

    def tables(e, carry):
        hit = qt[pl.ds(e, 1), :] == slot_no
        rows = pl.ds(pl.multiple_of(e * CAP, 16), CAP)
        onehot[rows, :] = jnp.where(hit, 1.0, 0.0).astype(BF16)
        combine_t[rows, :] = jnp.where(hit, wt[pl.ds(e, 1), :], 0.0).astype(BF16)
        return carry

    lax.fori_loop(0, EXPERTS, tables, 0)

    loads[2].wait()

    def norm(i, carry):
        rows = pl.ds(pl.multiple_of(i * 32, 32), 32)
        full = tok_v[rows, :].astype(F32)
        scale = lax.rsqrt(jnp.mean(full * full, axis=1, keepdims=True) + norm_eps)
        mine = tok_v[rows, pl.ds(pl.multiple_of(tp * COLS, COLS), COLS)].astype(F32)
        normed[rows, :] = (mine * scale).astype(BF16)
        return carry

    lax.fori_loop(0, ROWS // 32, norm, 0)

    def fill(i, carry):
        rows = pl.ds(pl.multiple_of(i * CHUNK, CHUNK), CHUNK)
        slots[rows, :] = jnp.dot(
            onehot[rows, :], normed[...], preferred_element_type=F32
        ).astype(BF16)
        return carry

    lax.fori_loop(0, CHUNKS, fill, 0)

    loads[3].wait()
    square = (OWN, OWN)
    gain = jnp.sum(
        jnp.where(
            lax.broadcasted_iota(jnp.int32, square, 0) == lax.broadcasted_iota(jnp.int32, square, 1),
            jnp.broadcast_to(gain_v[...], square), 0.0,
        ),
        axis=1, keepdims=True,
    )
    for i in (4, 5, 6):
        loads[i].wait()

    def fold(e, carry):
        gate, up = (gain * gate_v[e]).astype(BF16), (gain * up_v[e]).astype(BF16)
        wb1a[e, :, 0:SIDE] = gate[:, :SIDE]
        wb1a[e, :, SIDE:COLS] = up[:, :SIDE]
        wb1b[e, :, 0:SIDE] = gate[:, SIDE:]
        wb1b[e, :, SIDE:COLS] = up[:, SIDE:]
        wb2[e] = down_v[e].astype(BF16)
        return carry

    lax.fori_loop(0, EXPERTS, fold, 0)
    own_rows = pl.ds(pl.multiple_of(me * OWN, OWN), OWN)
    rcv1a[own_rows, :] = wb1a[fs]
    rcv1b[own_rows, :] = wb1b[fs]
    rcv2[own_rows, :] = wb2[fs]

    def slot_rows(e):
        return pl.ds(pl.multiple_of(e * CAP, 16), CAP)

    self_slot = 3 * 4 + y
    ag1[tp, slot_rows(self_slot), :] = slots[slot_rows(fs), :]

    pl.semaphore_wait(barrier, ZS * YS - 1 + 3)

    def send_slots(zt, yt, group):
        e = rem(zt, 4) * 4 + yt
        remote(
            slots.at[slot_rows(e)], ag1.at[tp, slot_rows(group * 4 + y)],
            tok_send, tok_recv.at[group], at(zt, yt),
        ).start()

    def same_plane(i, carry):
        send_slots(z, rem(y + i, YS), 3)
        return carry

    lax.fori_loop(1, YS, same_plane, 0)

    def one_away(yt, carry):
        send_slots(rem(z + 1, ZS), yt, 1)
        send_slots(rem(z + 7, ZS), yt, 2)
        return carry

    lax.fori_loop(0, YS, one_away, 0)

    def two_away(yt, carry):
        step = jnp.where(rem(y + yt, 2) == 0, 2, 6)
        send_slots(rem(z + step, ZS), yt, 0)
        return carry

    lax.fori_loop(0, YS, two_away, 0)

    def plane(k):
        away = (k + 1) // 2
        return rem(z + jnp.where(rem(k, 2) == 1, away, ZS - away), ZS)

    def send_weights(source, landing, send, recv):
        def one(i, carry):
            zt, yt = plane(i // 4), rem(y + rem(i, 4), YS)
            remote(
                source.at[rem(zt, 4) * 4 + yt], landing.at[own_rows],
                send, recv.at[z], at(zt, yt),
            ).start()
            return carry

        lax.fori_loop(1, ZS * YS, one, 0)

    send_weights(wb1a, rcv1a, w_send.at[0], w1a_recv)
    send_weights(wb1b, rcv1b, w_send.at[1], w1b_recv)
    send_weights(wb2, rcv2, w_send.at[2], w2_recv)

    def gather(buf, columns, send, recv):
        def piece(xx, cc, start, size):
            return buf.at[xx * 2 + cc, pl.ds(start, size), columns]

        def own(q):
            mine = piece(x, core, q * CHUNK, CHUNK)
            remote(mine, mine, send, recv.at[0, q], right).start()
            remote(mine, mine, send, recv.at[1, q], left).start()
            remote(mine, mine, send, recv.at[4, q], sib).start()

        def forward(q):
            whole = piece(x_left, core, q * CHUNK, CHUNK)
            landed(whole, recv.at[0, q])
            first = piece(x_left, core, q * CHUNK, HALF)
            remote(first, first, send, recv.at[2, q], right).start()
            remote(whole, whole, send, recv.at[5, q], sib).start()
            whole = piece(x_right, core, q * CHUNK, CHUNK)
            landed(whole, recv.at[1, q])
            second = piece(x_right, core, q * CHUNK + HALF, HALF)
            remote(second, second, send, recv.at[3, q], left).start()
            remote(whole, whole, send, recv.at[6, q], sib).start()

        def far(q):
            landed(piece(x_far, core, q * CHUNK, HALF), recv.at[2, q])
            landed(piece(x_far, core, q * CHUNK + HALF, HALF), recv.at[3, q])
            whole = piece(x_far, core, q * CHUNK, CHUNK)
            remote(whole, whole, send, recv.at[7, q], sib).start()

        def others(q):
            for i, xx in ((4, x), (5, x_left), (6, x_right), (7, x_far)):
                landed(piece(xx, 1 - core, q * CHUNK, CHUNK), recv.at[i, q])

        def run(order, prepare):
            for i in range(CHUNKS + 3):
                if i < CHUNKS:
                    prepare(order[i])
                    own(order[i])
                if 0 <= i - 2 < CHUNKS:
                    forward(order[i - 2])
                if 0 <= i - 4:
                    far(order[i - 4])
            far(order[CHUNKS - 1])
            for q in range(CHUNKS):
                others(q)

        return run

    def group_landed(q):
        landed(ag1.at[0, pl.ds(0, (3 if q == 3 else 4) * CAP)], tok_recv.at[q])

    gather(ag1, pl.ds(0, COLS), ag_send.at[0], ag1_recv)((3, 1, 2, 0), group_landed)

    def planes_landed(landing, recv, first, end):
        if first == 0:
            landed(landing.at[pl.ds(0, 3 * OWN)], recv.at[z])

        def one(k, carry):
            landed(landing.at[pl.ds(0, 4 * OWN)], recv.at[plane(k)])
            return carry

        lax.fori_loop(max(first, 1), end, one, 0)

    def product(left_of, right_of, rows, ks):
        total = None
        for k in ks:
            j = plane(k) if isinstance(ks, tuple) else k
            start = pl.multiple_of(j * COLS, COLS) if isinstance(ks, tuple) else k * COLS
            part = jnp.dot(
                left_of[j, rows, :], right_of[pl.ds(start, COLS), :], preferred_element_type=F32
            )
            total = part if total is None else total + part
        return total

    def half(landing, side, send, recv, hidden_recv):
        columns = pl.ds(side * SIDE, SIDE)

        def hidden(q):
            rows = pl.ds(q * CHUNK, CHUNK)
            pre = product(ag1, landing, rows, range(ZS))
            g = jnp.minimum(pre[:, :SIDE], clamp_limit)
            v = jnp.clip(pre[:, SIDE:], -clamp_limit, clamp_limit)
            ag2[tp, rows, columns] = (g * jax.nn.sigmoid(sigmoid_slope * g) * (v + 1.0)).astype(BF16)

        planes_landed(landing, recv, 0, ZS)
        gather(ag2, columns, send, hidden_recv)(tuple(range(CHUNKS)), hidden)

    half(rcv1a, 0, ag_send.at[1], w1a_recv, ag2a_recv)
    half(rcv1b, 1, ag_send.at[2], w1b_recv, ag2b_recv)

    def send_back(group, ys, zs):
        remote(
            res.at[slot_rows(group * 4 + ys)], ret.at[slot_rows(fs)],
            ret_send, ret_recv, at(zs, ys),
        ).start()

    def back(group):
        def one(i, carry):
            if group == 0:
                step = jnp.where(rem(y + i, 2) == 0, 6, 2)
                send_back(0, i, rem(z + step, ZS))
            elif group < 3:
                send_back(group, i, rem(z + (7 if group == 1 else 1), ZS))
            else:
                send_back(3, rem(y + i, YS), z)
            return carry

        lax.fori_loop(1 if group == 3 else 0, YS, one, 0)

    planes_landed(rcv2, w2_recv, 0, EARLY)

    def begin(r, carry):
        rows = pl.ds(pl.multiple_of(r * CHUNK, CHUNK), CHUNK)
        acc[rows, :] = product(ag2, rcv2, rows, tuple(range(EARLY)))
        return carry

    lax.fori_loop(0, CHUNKS, begin, 0)
    planes_landed(rcv2, w2_recv, EARLY, ZS)
    for r in range(CHUNKS):
        rows = pl.ds(r * CHUNK, CHUNK)
        res[rows, :] = (acc[rows, :] + product(ag2, rcv2, rows, tuple(range(EARLY, ZS)))).astype(BF16)
        back(r)
    ret[slot_rows(fs), :] = res[slot_rows(self_slot), :]

    landed(ret.at[pl.ds(0, SLOTS - CAP)], ret_recv)
    landed(slots.at[pl.ds(0, SLOTS - CAP)], tok_send)
    landed(ret.at[pl.ds(0, SLOTS - CAP)], ret_send)
    for i, landing in enumerate((rcv1a, rcv1b, rcv2)):
        landed(landing.at[pl.ds(0, 31 * OWN)], w_send.at[i])
    landed(ag1.at[pl.ds(0, 7)], ag_send.at[0])
    landed(ag2.at[pl.ds(0, 7), :, pl.ds(0, SIDE)], ag_send.at[1])
    landed(ag2.at[pl.ds(0, 7), :, pl.ds(0, SIDE)], ag_send.at[2])


def write_out(rcv1a, rcv1b, rcv2, ret, combine_t, og, ou, od, om, mix_v, sem):
    low, high = pl.ds(0, SIDE), pl.ds(SIDE, SIDE)
    copies = [
        pltpu.make_async_copy(s, d, sem.at[i])
        for i, (s, d) in enumerate((
            (rcv1a.at[:, low], og.at[0, :, low]), (rcv1b.at[:, low], og.at[0, :, high]),
            (rcv1a.at[:, high], ou.at[0, :, low]), (rcv1b.at[:, high], ou.at[0, :, high]),
            (rcv2, od.at[0]),
        ))
    ]
    for c in copies:
        c.start()
    mix_v[...] = lax.dot_general(
        combine_t[...], ret[...], (((0,), (0,)), ((), ())), preferred_element_type=F32
    ).astype(BF16)
    mix_out = pltpu.make_async_copy(mix_v, om, sem.at[5])
    mix_out.start()
    for c in copies:
        c.wait()
    mix_out.wait()


def local(tokens, route_ids, route_scores, norm_gain, gate_weight, up_weight, down_weight):
    hbm, vmem = pl.BlockSpec(memory_space=pltpu.HBM), pl.BlockSpec(memory_space=pltpu.VMEM)
    dma = pltpu.SemaphoreType.DMA
    rows = jax.ShapeDtypeStruct((2048, COLS), BF16)
    slots = jax.ShapeDtypeStruct((SLOTS, COLS), BF16)
    landed = pl.pallas_call(
        kernel,
        name="hand_over",
        out_shape=(rows, rows, rows, slots, slots),
        in_specs=[hbm] * 7,
        out_specs=[vmem] * 5,
        scratch_shapes=[
            pltpu.VMEM((ROWS, 2048), BF16),
            pltpu.VMEM((TOP, ROWS), jnp.int32),
            pltpu.VMEM((TOP, ROWS), F32),
            pltpu.VMEM((1, OWN), F32),
            pltpu.VMEM((EXPERTS, OWN, COLS), F32),
            pltpu.VMEM((EXPERTS, OWN, COLS), F32),
            pltpu.VMEM((EXPERTS, OWN, COLS), F32),
            pltpu.VMEM((EXPERTS, ROWS), F32),
            pltpu.VMEM((EXPERTS, ROWS), F32),
            pltpu.VMEM((SLOTS, ROWS), BF16),
            pltpu.VMEM((ROWS, COLS), BF16),
            pltpu.VMEM((SLOTS, COLS), BF16),
            pltpu.VMEM((EXPERTS, OWN, COLS), BF16),
            pltpu.VMEM((EXPERTS, OWN, COLS), BF16),
            pltpu.VMEM((EXPERTS, OWN, COLS), BF16),
            pltpu.VMEM((TPS, SLOTS, COLS), BF16),
            pltpu.VMEM((TPS, SLOTS, COLS), BF16),
            pltpu.VMEM((SLOTS, COLS), F32),
            pltpu.VMEM((SLOTS, COLS), BF16),
            dma((7,)), dma(()), dma((4,)), dma((3,)), dma((ZS,)), dma((ZS,)), dma((ZS,)),
            dma((3,)), dma((8, CHUNKS)), dma((8, CHUNKS)), dma((8, CHUNKS)), dma(()), dma(()),
        ],
        compiler_params=pltpu.CompilerParams(
            collective_id=0, has_side_effects=True, vmem_limit_bytes=52 * 1000 * 1000
        ),
    )(
        *(
            pltpu.with_memory_space_constraint(a, pltpu.HBM)
            for a in (tokens, route_ids.T, route_scores.T, norm_gain.reshape(1, OWN),
                      gate_weight, up_weight, down_weight)
        )
    )
    served = jax.ShapeDtypeStruct((1, 2048, COLS), BF16)
    return pl.pallas_call(
        write_out,
        name="write_out",
        out_shape=(served, served, served, jax.ShapeDtypeStruct((ROWS, COLS), BF16)),
        in_specs=[vmem] * 5,
        out_specs=[hbm] * 4,
        scratch_shapes=[pltpu.VMEM((ROWS, COLS), BF16), dma((6,))],
        compiler_params=pltpu.CompilerParams(vmem_limit_bytes=12 * 1024 * 1024),
    )(*landed)


def solution(mesh):
    in_specs = (
        P(("gr", "fs"), None),
        P(("gr", "fs"), None),
        P(("gr", "fs"), None),
        P(("gr", "fs")),
        P(None, ("gr", "fs"), "tp"),
        P(None, ("gr", "fs"), "tp"),
        P(None, ("gr", "fs"), "tp"),
    )
    out_specs = (
        P("fs", None, "tp"),
        P("fs", None, "tp"),
        P("fs", None, "tp"),
        P(("gr", "fs"), "tp"),
    )
    return jax.shard_map(local, mesh=mesh, in_specs=in_specs, out_specs=out_specs, check_vma=False)
```

```python
import jax
import jax.numpy as jnp
from jax import lax
from jax.experimental import pallas as pl
from jax.experimental.pallas import tpu as pltpu
from jax.sharding import PartitionSpec as P

MESH = pl.DeviceIdType.MESH
BF16, F32 = jnp.bfloat16, jnp.float32

EXPERTS = 16
TOP = 4
CAP = 80
ROWS = 256
SLOTS = EXPERTS * CAP
COLS = 256
SIDE = COLS // 2
TPS = 8
ZS, YS, XS = 8, 4, 4
OWN = 64
CHUNKS = 4
CHUNK = SLOTS // CHUNKS
HALF = CHUNK // 2
EARLY = 5

norm_eps = 1e-06
clamp_limit = 7.0
sigmoid_slope = 1.702


SEQ = [7, 5, 6, 3, 4, 1, 2, 0]
FIRST, LATER = SEQ[:EARLY], SEQ[EARLY:]
ORDER = [(k, d) for d in (2, 1, 3, 0) for k in SEQ if k or d]


def rem(a, n):
    return lax.rem(a, n)


def kernel(
    tok_h, ids_h, sc_h, gain_h, gate_h, up_h, down_h,
    rcv1a, rcv1b, rcv2, ret, combine_t,
    tok_v, ids_v, sc_v, gain_v, gate_v, up_v, down_v,
    qt, wt, onehot, normed, slots,
    wb1a, wb1b, wb2, ag1, ag2, acc, res,
    load_sem, tok_send, tok_recv, w_send, w_recv,
    ag_send, ag1_recv, ag2a_recv, ag2b_recv, sib_recv, ret_send, ret_recv,
):
    gr, fs, tp = lax.axis_index("gr"), lax.axis_index("fs"), lax.axis_index("tp")
    z, y = gr * 4 + fs // 4, rem(fs, 4)
    x, core = tp // 2, rem(tp, 2)
    me = z * YS + y

    def along(xx, cc):
        return (gr, fs, xx * 2 + cc)

    x_right, x_left, x_far = rem(x + 1, XS), rem(x + 3, XS), rem(x + 2, XS)
    right, left, sib = along(x_right, core), along(x_left, core), along(x, 1 - core)

    def remote(src, dst, send, recv, device):
        return pltpu.make_async_remote_copy(
            src_ref=src, dst_ref=dst, send_sem=send, recv_sem=recv,
            device_id=device, device_id_type=MESH,
        )

    def landed(ref, sem):
        pltpu.make_async_copy(ref, ref, sem).wait()

    planes = [rem(z + (away % ZS), ZS) for away in (0, 1, -1, 2, -2, 3, -3, 4)]
    plane_gr, plane_fs = [p // 4 for p in planes], [rem(p, 4) * 4 for p in planes]
    row = [y] + [rem(y + d, YS) for d in range(1, YS)]
    peers = [(k, d) for k in range(ZS) for d in range(YS)][1:]

    def peer(k, d):
        return (plane_gr[k], plane_fs[k] + row[d], tp)

    barrier = pltpu.get_barrier_semaphore()
    for k, d in peers[::-1]:
        pl.semaphore_signal(barrier, inc=1, device_id=peer(k, d), device_id_type=MESH)
    for d in (right, left, sib):
        pl.semaphore_signal(barrier, inc=1, device_id=d, device_id_type=MESH)

    loads = [
        pltpu.make_async_copy(s, d, load_sem.at[i])
        for i, (s, d) in enumerate(
            ((ids_h, ids_v), (sc_h, sc_v), (tok_h, tok_v), (gain_h, gain_v),
             (gate_h, gate_v), (up_h, up_v), (down_h, down_v))
        )
    ]
    for c in loads:
        c.start()

    loads[0].wait()
    loads[1].wait()
    ids = ids_v[...]
    exponent = jnp.exp(sc_v[...])
    total = jnp.sum(exponent, axis=0, keepdims=True)
    weights = (exponent / total).astype(BF16).astype(F32)
    expert_of = lax.broadcasted_iota(jnp.int32, (EXPERTS, ROWS), 0)
    member = jnp.zeros((EXPERTS, ROWS), F32)
    weight_of = jnp.zeros((EXPERTS, ROWS), F32)
    for k in range(TOP):
        same = ids[k : k + 1, :] == expert_of
        member = member + jnp.where(same, 1.0, 0.0)
        weight_of = weight_of + jnp.where(same, weights[k : k + 1, :], 0.0)
    earlier = jnp.where(
        lax.broadcasted_iota(jnp.int32, (ROWS, ROWS), 0)
        < lax.broadcasted_iota(jnp.int32, (ROWS, ROWS), 1),
        1.0, 0.0,
    ).astype(BF16)
    before = jnp.dot(member.astype(BF16), earlier, preferred_element_type=F32)
    qt[...] = jnp.where(member > 0.5, before, -1.0)
    wt[...] = weight_of

    slot_no = lax.broadcasted_iota(jnp.int32, (CAP, ROWS), 0).astype(F32)

    def tables(e, carry):
        hit = qt[pl.ds(e, 1), :] == slot_no
        rows = pl.ds(pl.multiple_of(e * CAP, 16), CAP)
        onehot[rows, :] = jnp.where(hit, 1.0, 0.0).astype(BF16)
        combine_t[rows, :] = jnp.where(hit, wt[pl.ds(e, 1), :], 0.0).astype(BF16)
        return carry

    lax.fori_loop(0, EXPERTS, tables, 0)

    loads[2].wait()

    def norm(i, carry):
        rows = pl.ds(pl.multiple_of(i * 32, 32), 32)
        full = tok_v[rows, :].astype(F32)
        scale = lax.rsqrt(jnp.mean(full * full, axis=1, keepdims=True) + norm_eps)
        mine = tok_v[rows, pl.ds(pl.multiple_of(tp * COLS, COLS), COLS)].astype(F32)
        normed[rows, :] = (mine * scale).astype(BF16)
        return carry

    lax.fori_loop(0, ROWS // 32, norm, 0)

    def fill(i, carry):
        rows = pl.ds(pl.multiple_of(i * CHUNK, CHUNK), CHUNK)
        slots[rows, :] = jnp.dot(
            onehot[rows, :], normed[...], preferred_element_type=F32
        ).astype(BF16)
        return carry

    lax.fori_loop(0, CHUNKS, fill, 0)

    loads[3].wait()
    square = (OWN, OWN)
    gain = jnp.sum(
        jnp.where(
            lax.broadcasted_iota(jnp.int32, square, 0) == lax.broadcasted_iota(jnp.int32, square, 1),
            jnp.broadcast_to(gain_v[...], square), 0.0,
        ),
        axis=1, keepdims=True,
    )
    for i in (4, 5, 6):
        loads[i].wait()

    def fold(e, carry):
        gate, up = (gain * gate_v[e]).astype(BF16), (gain * up_v[e]).astype(BF16)
        wb1a[e, :, 0:SIDE] = gate[:, :SIDE]
        wb1a[e, :, SIDE:COLS] = up[:, :SIDE]
        wb1b[e, :, 0:SIDE] = gate[:, SIDE:]
        wb1b[e, :, SIDE:COLS] = up[:, SIDE:]
        wb2[e] = down_v[e].astype(BF16)
        return carry

    lax.fori_loop(0, EXPERTS, fold, 0)
    own_rows = pl.ds(pl.multiple_of(me * OWN, OWN), OWN)
    rcv1a[own_rows, :] = wb1a[fs]
    rcv1b[own_rows, :] = wb1b[fs]
    rcv2[own_rows, :] = wb2[fs]

    def slot_rows(e):
        return pl.ds(pl.multiple_of(e * CAP, 16), CAP)

    self_slot = 3 * 4 + y
    ag1[tp, slot_rows(self_slot), :] = slots[slot_rows(fs), :]

    pl.semaphore_wait(barrier, ZS * YS - 1 + 3)

    def routes(group):
        if group == 3:
            return [(0, d) for d in range(1, YS)]
        if group == 0:
            return [(3 + d % 2, d) for d in range(YS)]
        return [(group, d) for d in range(YS)]

    for group in (3, 1, 2, 0):
        for k, d in routes(group):
            remote(
                slots.at[slot_rows(plane_fs[k] + row[d])], ag1.at[tp, slot_rows(group * 4 + y)],
                tok_send, tok_recv.at[group], peer(k, d),
            ).start()

    def send_weights(source, landing, columns, send, recv):
        for k, d in ORDER:
            remote(
                source.at[plane_fs[k] + row[d], :, columns], landing.at[own_rows, columns],
                send, recv(k), peer(k, d),
            ).start()

    whole, low, high = pl.ds(0, COLS), pl.ds(0, SIDE), pl.ds(SIDE, SIDE)
    send_weights(wb1a, rcv1a, whole, w_send.at[0], lambda k: w_recv.at[0])
    send_weights(wb1b, rcv1b, whole, w_send.at[1], lambda k: w_recv.at[1])
    send_weights(wb2, rcv2, low, w_send.at[2], lambda k: w_recv.at[2])
    send_weights(wb2, rcv2, high, w_send.at[3], lambda k: w_recv.at[3 if k in FIRST else 4])

    def gather(buf, columns, send, recv, sib_recv):
        def piece(xx, cc, start, size):
            return buf.at[xx * 2 + cc, pl.ds(start, size), columns]

        def own(q):
            mine = piece(x, core, q * CHUNK, CHUNK)
            remote(mine, mine, send, recv.at[0, q], right).start()
            remote(mine, mine, send, recv.at[1, q], left).start()
            remote(mine, mine, send, sib_recv, sib).start()

        def forward(q):
            whole = piece(x_left, core, q * CHUNK, CHUNK)
            landed(whole, recv.at[0, q])
            first = piece(x_left, core, q * CHUNK, HALF)
            remote(first, first, send, recv.at[2, q], right).start()
            remote(whole, whole, send, sib_recv, sib).start()
            whole = piece(x_right, core, q * CHUNK, CHUNK)
            landed(whole, recv.at[1, q])
            second = piece(x_right, core, q * CHUNK + HALF, HALF)
            remote(second, second, send, recv.at[2, q], left).start()
            remote(whole, whole, send, sib_recv, sib).start()

        def far(q):
            both = piece(x_far, core, q * CHUNK, CHUNK)
            landed(both, recv.at[2, q])
            remote(both, both, send, sib_recv, sib).start()

        def run(order, prepare):
            for i in range(CHUNKS + 3):
                if i < CHUNKS:
                    prepare(order[i])
                    own(order[i])
                if 0 <= i - 2 < CHUNKS:
                    forward(order[i - 2])
                if 0 <= i - 4:
                    far(order[i - 4])
            far(order[CHUNKS - 1])
            landed(buf.at[pl.ds(0, 4), :, columns], sib_recv)

        return run

    def group_landed(q):
        landed(ag1.at[0, pl.ds(0, (3 if q == 3 else 4) * CAP)], tok_recv.at[q])

    gather(ag1, whole, ag_send.at[0], ag1_recv, sib_recv.at[0])((3, 1, 2, 0), group_landed)

    def product(left_of, right_of, rows, columns, ks):
        total = None
        for k in ks:
            j = planes[k] if isinstance(ks, tuple) else k
            start = pl.multiple_of(j * COLS, COLS) if isinstance(ks, tuple) else k * COLS
            part = jnp.dot(
                left_of[j, rows, :], right_of[pl.ds(start, COLS), columns],
                preferred_element_type=F32,
            )
            total = part if total is None else total + part
        return total

    def half(landing, side, columns, hidden_recv):
        def hidden(q):
            rows = pl.ds(q * CHUNK, CHUNK)
            pre = product(ag1, landing, rows, whole, range(ZS))
            g = jnp.minimum(pre[:, :SIDE], clamp_limit)
            v = jnp.clip(pre[:, SIDE:], -clamp_limit, clamp_limit)
            ag2[tp, rows, columns] = (g * jax.nn.sigmoid(sigmoid_slope * g) * (v + 1.0)).astype(BF16)

        landed(landing.at[pl.ds(0, 31 * OWN)], w_recv.at[side])
        gather(ag2, columns, ag_send.at[1 + side], hidden_recv, sib_recv.at[1 + side])(
            tuple(range(CHUNKS)), hidden
        )

    half(rcv1a, 0, low, ag2a_recv)
    half(rcv1b, 1, high, ag2b_recv)

    def back(group, side, columns):
        for k, d in routes(group):
            away = (0, 2, 1, 4, 3)[k]
            remote(
                res.at[slot_rows(group * 4 + row[d]), columns], ret.at[slot_rows(fs), columns],
                ret_send.at[side], ret_recv.at[side], peer(away, d),
            ).start()

    landed(rcv2.at[pl.ds(0, 31 * OWN), low], w_recv.at[2])
    for r in range(CHUNKS):
        rows = pl.ds(r * CHUNK, CHUNK)
        res[rows, low] = product(ag2, rcv2, rows, low, range(ZS)).astype(BF16)
        back(r, 0, low)

    landed(rcv2.at[pl.ds(0, (4 * EARLY - (0 in FIRST)) * OWN), high], w_recv.at[3])

    def begin(r, carry):
        rows = pl.ds(pl.multiple_of(r * CHUNK, CHUNK), CHUNK)
        acc[rows, :] = product(ag2, rcv2, rows, high, tuple(FIRST))
        return carry

    lax.fori_loop(0, CHUNKS, begin, 0)
    landed(rcv2.at[pl.ds(0, (4 * (ZS - EARLY) - (0 in LATER)) * OWN), high], w_recv.at[4])
    for r in range(CHUNKS):
        rows = pl.ds(r * CHUNK, CHUNK)
        late = product(ag2, rcv2, rows, high, tuple(LATER))
        res[rows, high] = (acc[rows, :] + late).astype(BF16)
        back(r, 1, high)
    ret[slot_rows(fs), :] = res[slot_rows(self_slot), :]

    landed(slots.at[pl.ds(0, SLOTS - CAP)], tok_send)
    for i, landing in enumerate((rcv1a, rcv1b, rcv2.at[:, low], rcv2.at[:, high])):
        landed(landing.at[pl.ds(0, 31 * OWN)], w_send.at[i])
    landed(ag1.at[pl.ds(0, 7)], ag_send.at[0])
    for side in range(2):
        landed(ag2.at[pl.ds(0, 7), :, pl.ds(0, SIDE)], ag_send.at[1 + side])
        landed(ret.at[pl.ds(0, SLOTS - CAP), pl.ds(0, SIDE)], ret_send.at[side])
    for side in range(2):
        landed(ret.at[pl.ds(0, SLOTS - CAP), pl.ds(side * SIDE, SIDE)], ret_recv.at[side])


def write_out(rcv1a, rcv1b, rcv2, ret, combine_t, og, ou, od, om, mix_v, sem):
    low, high = pl.ds(0, SIDE), pl.ds(SIDE, SIDE)
    copies = [
        pltpu.make_async_copy(s, d, sem.at[i])
        for i, (s, d) in enumerate((
            (rcv1a.at[:, low], og.at[0, :, low]), (rcv1b.at[:, low], og.at[0, :, high]),
            (rcv1a.at[:, high], ou.at[0, :, low]), (rcv1b.at[:, high], ou.at[0, :, high]),
            (rcv2, od.at[0]),
        ))
    ]
    for c in copies:
        c.start()
    mix_v[...] = lax.dot_general(
        combine_t[...], ret[...], (((0,), (0,)), ((), ())), preferred_element_type=F32
    ).astype(BF16)
    mix_out = pltpu.make_async_copy(mix_v, om, sem.at[5])
    mix_out.start()
    for c in copies:
        c.wait()
    mix_out.wait()


def local(tokens, route_ids, route_scores, norm_gain, gate_weight, up_weight, down_weight):
    hbm, vmem = pl.BlockSpec(memory_space=pltpu.HBM), pl.BlockSpec(memory_space=pltpu.VMEM)
    dma = pltpu.SemaphoreType.DMA
    rows = jax.ShapeDtypeStruct((2048, COLS), BF16)
    slots = jax.ShapeDtypeStruct((SLOTS, COLS), BF16)
    landed = pl.pallas_call(
        kernel,
        name="hand_over",
        out_shape=(rows, rows, rows, slots, slots),
        in_specs=[hbm] * 7,
        out_specs=[vmem] * 5,
        scratch_shapes=[
            pltpu.VMEM((ROWS, 2048), BF16),
            pltpu.VMEM((TOP, ROWS), jnp.int32),
            pltpu.VMEM((TOP, ROWS), F32),
            pltpu.VMEM((1, OWN), F32),
            pltpu.VMEM((EXPERTS, OWN, COLS), F32),
            pltpu.VMEM((EXPERTS, OWN, COLS), F32),
            pltpu.VMEM((EXPERTS, OWN, COLS), F32),
            pltpu.VMEM((EXPERTS, ROWS), F32),
            pltpu.VMEM((EXPERTS, ROWS), F32),
            pltpu.VMEM((SLOTS, ROWS), BF16),
            pltpu.VMEM((ROWS, COLS), BF16),
            pltpu.VMEM((SLOTS, COLS), BF16),
            pltpu.VMEM((EXPERTS, OWN, COLS), BF16),
            pltpu.VMEM((EXPERTS, OWN, COLS), BF16),
            pltpu.VMEM((EXPERTS, OWN, COLS), BF16),
            pltpu.VMEM((TPS, SLOTS, COLS), BF16),
            pltpu.VMEM((TPS, SLOTS, COLS), BF16),
            pltpu.VMEM((SLOTS, SIDE), F32),
            pltpu.VMEM((SLOTS, COLS), BF16),
            dma((7,)), dma(()), dma((4,)), dma((4,)), dma((5,)),
            dma((3,)), dma((3, CHUNKS)), dma((3, CHUNKS)), dma((3, CHUNKS)), dma((3,)),
            dma((2,)), dma((2,)),
        ],
        compiler_params=pltpu.CompilerParams(
            collective_id=0, has_side_effects=True, vmem_limit_bytes=44 * 1024 * 1024
        ),
    )(
        *(
            pltpu.with_memory_space_constraint(a, pltpu.HBM)
            for a in (tokens, route_ids.T, route_scores.T, norm_gain.reshape(1, OWN),
                      gate_weight, up_weight, down_weight)
        )
    )
    served = jax.ShapeDtypeStruct((1, 2048, COLS), BF16)
    return pl.pallas_call(
        write_out,
        name="write_out",
        out_shape=(served, served, served, jax.ShapeDtypeStruct((ROWS, COLS), BF16)),
        in_specs=[vmem] * 5,
        out_specs=[hbm] * 4,
        scratch_shapes=[pltpu.VMEM((ROWS, COLS), BF16), dma((6,))],
        compiler_params=pltpu.CompilerParams(vmem_limit_bytes=12 * 1024 * 1024),
    )(*landed)


def solution(mesh):
    in_specs = (
        P(("gr", "fs"), None),
        P(("gr", "fs"), None),
        P(("gr", "fs"), None),
        P(("gr", "fs")),
        P(None, ("gr", "fs"), "tp"),
        P(None, ("gr", "fs"), "tp"),
        P(None, ("gr", "fs"), "tp"),
    )
    out_specs = (
        P("fs", None, "tp"),
        P("fs", None, "tp"),
        P("fs", None, "tp"),
        P(("gr", "fs"), "tp"),
    )
    return jax.shard_map(local, mesh=mesh, in_specs=in_specs, out_specs=out_specs, check_vma=False)
```

```python
import jax
import jax.numpy as jnp
from jax import lax
from jax.experimental import pallas as pl
from jax.experimental.pallas import tpu as pltpu
from jax.sharding import PartitionSpec as P

MESH = pl.DeviceIdType.MESH
BF16, F32 = jnp.bfloat16, jnp.float32

EXPERTS = 16
TOP = 4
CAP = 80
ROWS = 256
SLOTS = EXPERTS * CAP
COLS = 256
SIDE = COLS // 2
TPS = 8
ZS, YS, XS = 8, 4, 4
OWN = 64
CHUNKS = 4
CHUNK = SLOTS // CHUNKS
HALF = CHUNK // 2
AHEAD = 6
EARLY = 5

norm_eps = 1e-06
clamp_limit = 7.0
sigmoid_slope = 1.702


SEQ = [7, 5, 6, 3, 4, 1, 2, 0]
FIRST, LATER = SEQ[:EARLY], SEQ[EARLY:]
ORDER = [(k, d) for d in (2, 1, 3, 0) for k in SEQ if k or d]


def rem(a, n):
    return lax.rem(a, n)


def kernel(
    tok_h, ids_h, sc_h, gain_h, gate_h, up_h, down_h,
    rcv1a, rcv1b, rcv2, ret, combine_t,
    tok_v, ids_v, sc_v, gain_v, gate_v, up_v, down_v,
    qt, wt, onehot, normed, slots, rows_in, ids_in,
    wb1a, wb1b, wb2, ag1, ag2, acc, res,
    load_sem, near_send, near_recv, tok_send, tok_recv, w_send, w_recv,
    ag_send, ag1_recv, ag2a_recv, ag2b_recv, sib_recv, ret_send, ret_recv,
):
    gr, fs, tp = lax.axis_index("gr"), lax.axis_index("fs"), lax.axis_index("tp")
    z, y = gr * 4 + fs // 4, rem(fs, 4)
    x, core = tp // 2, rem(tp, 2)
    me = z * YS + y

    def along(xx, cc):
        return (gr, fs, xx * 2 + cc)

    x_right, x_left, x_far = rem(x + 1, XS), rem(x + 3, XS), rem(x + 2, XS)
    right, left, sib = along(x_right, core), along(x_left, core), along(x, 1 - core)

    def remote(src, dst, send, recv, device):
        return pltpu.make_async_remote_copy(
            src_ref=src, dst_ref=dst, send_sem=send, recv_sem=recv,
            device_id=device, device_id_type=MESH,
        )

    def landed(ref, sem):
        pltpu.make_async_copy(ref, ref, sem).wait()

    planes = [rem(z + (away % ZS), ZS) for away in (0, 1, -1, 2, -2, 3, -3, 4)]
    plane_gr, plane_fs = [p // 4 for p in planes], [rem(p, 4) * 4 for p in planes]
    row = [y] + [rem(y + d, YS) for d in range(1, YS)]
    peers = [(k, d) for k in range(ZS) for d in range(YS)][1:]

    def peer(k, d):
        return (plane_gr[k], plane_fs[k] + row[d], tp)

    barrier = pltpu.get_barrier_semaphore()
    for k, d in peers[::-1]:
        pl.semaphore_signal(barrier, inc=1, device_id=peer(k, d), device_id_type=MESH)
    for d in (right, left, sib):
        pl.semaphore_signal(barrier, inc=1, device_id=d, device_id_type=MESH)

    loads = [
        pltpu.make_async_copy(s, d, load_sem.at[i])
        for i, (s, d) in enumerate(
            ((ids_h, ids_v), (sc_h, sc_v), (tok_h, tok_v), (gain_h, gain_v),
             (gate_h, gate_v), (up_h, up_v), (down_h, down_v))
        )
    ]
    for c in loads:
        c.start()

    expert_of = lax.broadcasted_iota(jnp.int32, (EXPERTS, ROWS), 0)
    earlier = jnp.where(
        lax.broadcasted_iota(jnp.int32, (ROWS, ROWS), 0)
        < lax.broadcasted_iota(jnp.int32, (ROWS, ROWS), 1),
        1.0, 0.0,
    ).astype(BF16)

    def slot_table(ids):
        member = jnp.zeros((EXPERTS, ROWS), F32)
        for k in range(TOP):
            member = member + jnp.where(ids[k : k + 1, :] == expert_of, 1.0, 0.0)
        before = jnp.dot(member.astype(BF16), earlier, preferred_element_type=F32)
        return jnp.where(member > 0.5, before, -1.0)

    slot_no = lax.broadcasted_iota(jnp.int32, (CAP, ROWS), 0).astype(F32)

    def fill(table, rows, experts, out):
        for i, e in enumerate(experts):
            hit = qt[table, pl.ds(e, 1), :] == slot_no
            onehot[i * CAP : (i + 1) * CAP, :] = jnp.where(hit, 1.0, 0.0).astype(BF16)
        n = len(experts) * CAP
        out[0:n, :] = jnp.dot(onehot[0:n, :], rows, preferred_element_type=F32).astype(BF16)

    loads[0].wait()
    qt[0] = slot_table(ids_v[...])

    loads[2].wait()

    def norm(i, carry):
        rows = pl.ds(pl.multiple_of(i * 32, 32), 32)
        full = tok_v[rows, :].astype(F32)
        scale = lax.rsqrt(jnp.mean(full * full, axis=1, keepdims=True) + norm_eps)
        mine = tok_v[rows, pl.ds(pl.multiple_of(tp * COLS, COLS), COLS)].astype(F32)
        normed[rows, :] = (mine * scale).astype(BF16)
        return carry

    lax.fori_loop(0, ROWS // 32, norm, 0)

    here = [plane_fs[0] + row[d] for d in range(YS)]
    slots_own = slots.at[0]
    fill(0, normed[...], here, slots_own)

    loads[3].wait()
    square = (OWN, OWN)
    gain = jnp.sum(
        jnp.where(
            lax.broadcasted_iota(jnp.int32, square, 0) == lax.broadcasted_iota(jnp.int32, square, 1),
            jnp.broadcast_to(gain_v[...], square), 0.0,
        ),
        axis=1, keepdims=True,
    )
    for i in (4, 5, 6):
        loads[i].wait()

    def fold(e, carry):
        gate, up = (gain * gate_v[e]).astype(BF16), (gain * up_v[e]).astype(BF16)
        wb1a[e, :, 0:SIDE] = gate[:, :SIDE]
        wb1a[e, :, SIDE:COLS] = up[:, :SIDE]
        wb1b[e, :, 0:SIDE] = gate[:, SIDE:]
        wb1b[e, :, SIDE:COLS] = up[:, SIDE:]
        wb2[e] = down_v[e].astype(BF16)
        return carry

    lax.fori_loop(0, EXPERTS, fold, 0)
    own_rows = pl.ds(pl.multiple_of(me * OWN, OWN), OWN)
    rcv1a[own_rows, :] = wb1a[fs]
    rcv1b[own_rows, :] = wb1b[fs]
    rcv2[own_rows, :] = wb2[fs]

    def slot_rows(e):
        return pl.ds(pl.multiple_of(e * CAP, 16), CAP)

    self_slot = 3 * 4 + y
    ag1[tp, slot_rows(self_slot), :] = slots_own[0:CAP, :]

    pl.semaphore_wait(barrier, ZS * YS - 1 + 3)

    def routes(group):
        if group == 3:
            return [(0, d) for d in range(1, YS)]
        if group == 0:
            return [(3 + d % 2, d) for d in range(YS)]
        return [(group, d) for d in range(YS)]

    up, below = peer(1, 0), peer(2, 0)
    for side, device in enumerate((up, below)):
        remote(normed, rows_in.at[side], near_send.at[0], near_recv.at[side], device).start()
        remote(ids_v, ids_in.at[side], near_send.at[1], near_recv.at[2 + side], device).start()

    def send_slots(side, i, group, k, d):
        remote(
            slots.at[side, pl.ds(i * CAP, CAP)], ag1.at[tp, slot_rows(group * 4 + y)],
            tok_send, tok_recv.at[group], peer(k, d),
        ).start()

    for d in range(1, YS):
        send_slots(0, d, 3, 0, d)

    def send_weights(source, landing, columns, send, recv, some=slice(None)):
        for k, d in ORDER[some]:
            remote(
                source.at[plane_fs[k] + row[d], :, columns], landing.at[own_rows, columns],
                send, recv(k), peer(k, d),
            ).start()

    whole, low, high = pl.ds(0, COLS), pl.ds(0, SIDE), pl.ds(SIDE, SIDE)
    send_weights(wb1a, rcv1a, whole, w_send.at[0], lambda k: w_recv.at[0], slice(0, AHEAD))

    loads[1].wait()
    ids, exponent = ids_v[...], jnp.exp(sc_v[...])
    total = jnp.sum(exponent, axis=0, keepdims=True)
    weights = (exponent / total).astype(BF16).astype(F32)
    weight_of = jnp.zeros((EXPERTS, ROWS), F32)
    for k in range(TOP):
        weight_of = weight_of + jnp.where(ids[k : k + 1, :] == expert_of, weights[k : k + 1, :], 0.0)
    wt[...] = weight_of

    def combine(e, carry):
        hit = qt[0, pl.ds(e, 1), :] == slot_no
        rows = pl.ds(pl.multiple_of(e * CAP, 16), CAP)
        combine_t[rows, :] = jnp.where(hit, wt[pl.ds(e, 1), :], 0.0).astype(BF16)
        return carry

    lax.fori_loop(0, EXPERTS, combine, 0)

    for side in range(2):
        landed(ids_in.at[side], near_recv.at[2 + side])
        landed(rows_in.at[side], near_recv.at[side])
        qt[1 + side] = slot_table(ids_in[side])
        beyond = [(1 + side, d) for d in range(side, YS, 2)]
        experts = here + [plane_fs[k] + row[d] for k, d in beyond]
        fill(1 + side, rows_in[side], experts, slots.at[1 + side])
        for i, (k, d) in enumerate(beyond):
            send_slots(1 + side, YS + i, 0, k, d)
        for d in range(1, YS):
            send_slots(1 + side, d, 1 + side, 0, d)
        ag1[tp, slot_rows((1 + side) * 4 + y), :] = slots[1 + side, 0:CAP, :]

    send_weights(wb1a, rcv1a, whole, w_send.at[0], lambda k: w_recv.at[0], slice(AHEAD, None))
    send_weights(wb1b, rcv1b, whole, w_send.at[1], lambda k: w_recv.at[1])
    send_weights(wb2, rcv2, low, w_send.at[2], lambda k: w_recv.at[2])
    send_weights(wb2, rcv2, high, w_send.at[3], lambda k: w_recv.at[3 if k in FIRST else 4])

    def gather(buf, columns, send, recv, sib_recv):
        def piece(xx, cc, start, size):
            return buf.at[xx * 2 + cc, pl.ds(start, size), columns]

        def own(q):
            mine = piece(x, core, q * CHUNK, CHUNK)
            remote(mine, mine, send, recv.at[0, q], right).start()
            remote(mine, mine, send, recv.at[1, q], left).start()
            remote(mine, mine, send, sib_recv, sib).start()

        def forward(q):
            whole = piece(x_left, core, q * CHUNK, CHUNK)
            landed(whole, recv.at[0, q])
            first = piece(x_left, core, q * CHUNK, HALF)
            remote(first, first, send, recv.at[2, q], right).start()
            remote(whole, whole, send, sib_recv, sib).start()
            whole = piece(x_right, core, q * CHUNK, CHUNK)
            landed(whole, recv.at[1, q])
            second = piece(x_right, core, q * CHUNK + HALF, HALF)
            remote(second, second, send, recv.at[2, q], left).start()
            remote(whole, whole, send, sib_recv, sib).start()

        def far(q):
            both = piece(x_far, core, q * CHUNK, CHUNK)
            landed(both, recv.at[2, q])
            remote(both, both, send, sib_recv, sib).start()

        def run(order, prepare):
            for i in range(CHUNKS + 3):
                if i < CHUNKS:
                    prepare(order[i])
                    own(order[i])
                if 0 <= i - 2 < CHUNKS:
                    forward(order[i - 2])
                if 0 <= i - 4:
                    far(order[i - 4])
            far(order[CHUNKS - 1])
            landed(buf.at[pl.ds(0, 4), :, columns], sib_recv)

        return run

    def group_landed(q):
        landed(ag1.at[0, pl.ds(0, (4 if q == 0 else 3) * CAP)], tok_recv.at[q])

    gather(ag1, whole, ag_send.at[0], ag1_recv, sib_recv.at[0])((3, 1, 2, 0), group_landed)

    def product(left_of, right_of, rows, columns, ks):
        total = None
        for k in ks:
            j = planes[k] if isinstance(ks, tuple) else k
            start = pl.multiple_of(j * COLS, COLS) if isinstance(ks, tuple) else k * COLS
            part = jnp.dot(
                left_of[j, rows, :], right_of[pl.ds(start, COLS), columns],
                preferred_element_type=F32,
            )
            total = part if total is None else total + part
        return total

    def half(landing, side, columns, hidden_recv):
        def hidden(q):
            rows = pl.ds(q * CHUNK, CHUNK)
            pre = product(ag1, landing, rows, whole, range(ZS))
            g = jnp.minimum(pre[:, :SIDE], clamp_limit)
            v = jnp.clip(pre[:, SIDE:], -clamp_limit, clamp_limit)
            ag2[tp, rows, columns] = (g * jax.nn.sigmoid(sigmoid_slope * g) * (v + 1.0)).astype(BF16)

        landed(landing.at[pl.ds(0, 31 * OWN)], w_recv.at[side])
        gather(ag2, columns, ag_send.at[1 + side], hidden_recv, sib_recv.at[1 + side])(
            tuple(range(CHUNKS)), hidden
        )

    half(rcv1a, 0, low, ag2a_recv)
    half(rcv1b, 1, high, ag2b_recv)

    def back(group, side, columns):
        for k, d in routes(group):
            away = (0, 2, 1, 4, 3)[k]
            remote(
                res.at[slot_rows(group * 4 + row[d]), columns], ret.at[slot_rows(fs), columns],
                ret_send.at[side], ret_recv.at[side], peer(away, d),
            ).start()

    landed(rcv2.at[pl.ds(0, 31 * OWN), low], w_recv.at[2])
    for r in range(CHUNKS):
        rows = pl.ds(r * CHUNK, CHUNK)
        res[rows, low] = product(ag2, rcv2, rows, low, range(ZS)).astype(BF16)
        back(r, 0, low)

    landed(rcv2.at[pl.ds(0, (4 * EARLY - (0 in FIRST)) * OWN), high], w_recv.at[3])

    def begin(r, carry):
        rows = pl.ds(pl.multiple_of(r * CHUNK, CHUNK), CHUNK)
        acc[rows, :] = product(ag2, rcv2, rows, high, tuple(FIRST))
        return carry

    lax.fori_loop(0, CHUNKS, begin, 0)
    landed(rcv2.at[pl.ds(0, (4 * (ZS - EARLY) - (0 in LATER)) * OWN), high], w_recv.at[4])
    for r in range(CHUNKS):
        rows = pl.ds(r * CHUNK, CHUNK)
        late = product(ag2, rcv2, rows, high, tuple(LATER))
        res[rows, high] = (acc[rows, :] + late).astype(BF16)
        back(r, 1, high)
    ret[slot_rows(fs), :] = res[slot_rows(self_slot), :]

    landed(ret.at[pl.ds(0, 13 * CAP)], tok_send)
    landed(rows_in, near_send.at[0])
    landed(ids_in, near_send.at[1])
    for i, landing in enumerate((rcv1a, rcv1b, rcv2.at[:, low], rcv2.at[:, high])):
        landed(landing.at[pl.ds(0, 31 * OWN)], w_send.at[i])
    landed(ag1.at[pl.ds(0, 7)], ag_send.at[0])
    for side in range(2):
        landed(ag2.at[pl.ds(0, 7), :, pl.ds(0, SIDE)], ag_send.at[1 + side])
        landed(ret.at[pl.ds(0, SLOTS - CAP), pl.ds(0, SIDE)], ret_send.at[side])
    for side in range(2):
        landed(ret.at[pl.ds(0, SLOTS - CAP), pl.ds(side * SIDE, SIDE)], ret_recv.at[side])


def write_out(rcv1a, rcv1b, rcv2, ret, combine_t, og, ou, od, om, mix_v, sem):
    low, high = pl.ds(0, SIDE), pl.ds(SIDE, SIDE)
    copies = [
        pltpu.make_async_copy(s, d, sem.at[i])
        for i, (s, d) in enumerate((
            (rcv1a.at[:, low], og.at[0, :, low]), (rcv1b.at[:, low], og.at[0, :, high]),
            (rcv1a.at[:, high], ou.at[0, :, low]), (rcv1b.at[:, high], ou.at[0, :, high]),
            (rcv2, od.at[0]),
        ))
    ]
    for c in copies:
        c.start()
    mix_v[...] = lax.dot_general(
        combine_t[...], ret[...], (((0,), (0,)), ((), ())), preferred_element_type=F32
    ).astype(BF16)
    mix_out = pltpu.make_async_copy(mix_v, om, sem.at[5])
    mix_out.start()
    for c in copies:
        c.wait()
    mix_out.wait()


def local(tokens, route_ids, route_scores, norm_gain, gate_weight, up_weight, down_weight):
    hbm, vmem = pl.BlockSpec(memory_space=pltpu.HBM), pl.BlockSpec(memory_space=pltpu.VMEM)
    dma = pltpu.SemaphoreType.DMA
    rows = jax.ShapeDtypeStruct((2048, COLS), BF16)
    slots = jax.ShapeDtypeStruct((SLOTS, COLS), BF16)
    landed = pl.pallas_call(
        kernel,
        name="hand_over",
        out_shape=(rows, rows, rows, slots, slots),
        in_specs=[hbm] * 7,
        out_specs=[vmem] * 5,
        scratch_shapes=[
            pltpu.VMEM((ROWS, 2048), BF16),
            pltpu.VMEM((TOP, ROWS), jnp.int32),
            pltpu.VMEM((TOP, ROWS), F32),
            pltpu.VMEM((1, OWN), F32),
            pltpu.VMEM((EXPERTS, OWN, COLS), F32),
            pltpu.VMEM((EXPERTS, OWN, COLS), F32),
            pltpu.VMEM((EXPERTS, OWN, COLS), F32),
            pltpu.VMEM((3, EXPERTS, ROWS), F32),
            pltpu.VMEM((EXPERTS, ROWS), F32),
            pltpu.VMEM((6 * CAP, ROWS), BF16),
            pltpu.VMEM((ROWS, COLS), BF16),
            pltpu.VMEM((3, 6 * CAP, COLS), BF16),
            pltpu.VMEM((2, ROWS, COLS), BF16),
            pltpu.VMEM((2, TOP, ROWS), jnp.int32),
            pltpu.VMEM((EXPERTS, OWN, COLS), BF16),
            pltpu.VMEM((EXPERTS, OWN, COLS), BF16),
            pltpu.VMEM((EXPERTS, OWN, COLS), BF16),
            pltpu.VMEM((TPS, SLOTS, COLS), BF16),
            pltpu.VMEM((TPS, SLOTS, COLS), BF16),
            pltpu.VMEM((SLOTS, SIDE), F32),
            pltpu.VMEM((SLOTS, COLS), BF16),
            dma((7,)), dma((2,)), dma((4,)), dma(()), dma((4,)), dma((4,)), dma((5,)),
            dma((3,)), dma((3, CHUNKS)), dma((3, CHUNKS)), dma((3, CHUNKS)), dma((3,)),
            dma((2,)), dma((2,)),
        ],
        compiler_params=pltpu.CompilerParams(
            collective_id=0, has_side_effects=True, vmem_limit_bytes=44 * 1024 * 1024
        ),
    )(
        *(
            pltpu.with_memory_space_constraint(a, pltpu.HBM)
            for a in (tokens, route_ids.T, route_scores.T, norm_gain.reshape(1, OWN),
                      gate_weight, up_weight, down_weight)
        )
    )
    served = jax.ShapeDtypeStruct((1, 2048, COLS), BF16)
    return pl.pallas_call(
        write_out,
        name="write_out",
        out_shape=(served, served, served, jax.ShapeDtypeStruct((ROWS, COLS), BF16)),
        in_specs=[vmem] * 5,
        out_specs=[hbm] * 4,
        scratch_shapes=[pltpu.VMEM((ROWS, COLS), BF16), dma((6,))],
        compiler_params=pltpu.CompilerParams(vmem_limit_bytes=12 * 1024 * 1024),
    )(*landed)


def solution(mesh):
    in_specs = (
        P(("gr", "fs"), None),
        P(("gr", "fs"), None),
        P(("gr", "fs"), None),
        P(("gr", "fs")),
        P(None, ("gr", "fs"), "tp"),
        P(None, ("gr", "fs"), "tp"),
        P(None, ("gr", "fs"), "tp"),
    )
    out_specs = (
        P("fs", None, "tp"),
        P("fs", None, "tp"),
        P("fs", None, "tp"),
        P(("gr", "fs"), "tp"),
    )
    return jax.shard_map(local, mesh=mesh, in_specs=in_specs, out_specs=out_specs, check_vma=False)
```

```python
import jax
import jax.numpy as jnp
from jax import lax
from jax.experimental import pallas as pl
from jax.experimental.pallas import tpu as pltpu
from jax.sharding import PartitionSpec as P

MESH = pl.DeviceIdType.MESH
BF16, F32 = jnp.bfloat16, jnp.float32

EXPERTS = 16
TOP = 4
CAP = 80
ROWS = 256
SLOTS = EXPERTS * CAP
COLS = 256
SIDE = COLS // 2
TPS = 8
ZS, YS, XS = 8, 4, 4
OWN = 64
CHUNKS = 4
CHUNK = SLOTS // CHUNKS
HALF = CHUNK // 2
AHEAD = 6

norm_eps = 1e-06
clamp_limit = 7.0
sigmoid_slope = 1.702


SEQ = [7, 5, 6, 3, 4, 1, 2, 0]
FIRST, LATER = [7, 5, 6, 3, 4], [1, 2, 0]
ORDER = [(k, d) for d in (2, 1, 3, 0) for k in SEQ if k or d]
LAST_ORDER = [(k, d) for k in FIRST + LATER for d in (2, 1, 3, 0) if k or d]


def rem(a, n):
    return lax.rem(a, n)


def kernel(
    tok_h, ids_h, sc_h, gain_h, gate_h, up_h, down_h,
    rcv1a, rcv1b, rcv2, ret, combine_t,
    tok_v, ids_v, sc_v, gain_v, gate_v, up_v, down_v,
    qt, wt, onehot, normed, slots, rows_in, ids_in,
    wb1a, wb1b, wb2, ag1, ag2, acc, res,
    load_sem, near_send, near_recv, tok_send, tok_recv, w_send, w_recv,
    ag_send, ag1_recv, ag2a_recv, ag2b_recv, sib_recv, ret_send, ret_recv,
):
    gr, fs, tp = lax.axis_index("gr"), lax.axis_index("fs"), lax.axis_index("tp")
    z, y = gr * 4 + fs // 4, rem(fs, 4)
    x, core = tp // 2, rem(tp, 2)
    me = z * YS + y

    def along(xx, cc):
        return (gr, fs, xx * 2 + cc)

    x_right, x_left, x_far = rem(x + 1, XS), rem(x + 3, XS), rem(x + 2, XS)
    right, left, sib = along(x_right, core), along(x_left, core), along(x, 1 - core)

    def remote(src, dst, send, recv, device):
        return pltpu.make_async_remote_copy(
            src_ref=src, dst_ref=dst, send_sem=send, recv_sem=recv,
            device_id=device, device_id_type=MESH,
        )

    def landed(ref, sem):
        pltpu.make_async_copy(ref, ref, sem).wait()

    planes = [rem(z + (away % ZS), ZS) for away in (0, 1, -1, 2, -2, 3, -3, 4)]
    plane_gr, plane_fs = [p // 4 for p in planes], [rem(p, 4) * 4 for p in planes]
    row = [y] + [rem(y + d, YS) for d in range(1, YS)]
    peers = [(k, d) for k in range(ZS) for d in range(YS)][1:]

    def peer(k, d):
        return (plane_gr[k], plane_fs[k] + row[d], tp)

    barrier = pltpu.get_barrier_semaphore()
    for k, d in peers[::-1]:
        pl.semaphore_signal(barrier, inc=1, device_id=peer(k, d), device_id_type=MESH)
    for d in (right, left, sib):
        pl.semaphore_signal(barrier, inc=1, device_id=d, device_id_type=MESH)

    loads = [
        pltpu.make_async_copy(s, d, load_sem.at[i])
        for i, (s, d) in enumerate(
            ((ids_h, ids_v), (sc_h, sc_v), (tok_h, tok_v), (gain_h, gain_v),
             (gate_h, gate_v), (up_h, up_v), (down_h, down_v))
        )
    ]
    for c in loads:
        c.start()

    expert_of = lax.broadcasted_iota(jnp.int32, (EXPERTS, ROWS), 0)
    earlier = jnp.where(
        lax.broadcasted_iota(jnp.int32, (ROWS, ROWS), 0)
        < lax.broadcasted_iota(jnp.int32, (ROWS, ROWS), 1),
        1.0, 0.0,
    ).astype(BF16)

    def slot_table(ids):
        member = jnp.zeros((EXPERTS, ROWS), F32)
        for k in range(TOP):
            member = member + jnp.where(ids[k : k + 1, :] == expert_of, 1.0, 0.0)
        before = jnp.dot(member.astype(BF16), earlier, preferred_element_type=F32)
        return jnp.where(member > 0.5, before, -1.0)

    slot_no = lax.broadcasted_iota(jnp.int32, (CAP, ROWS), 0).astype(F32)

    def fill(table, rows, experts, out):
        for i, e in enumerate(experts):
            hit = qt[table, pl.ds(e, 1), :] == slot_no
            onehot[i * CAP : (i + 1) * CAP, :] = jnp.where(hit, 1.0, 0.0).astype(BF16)
        n = len(experts) * CAP
        out[0:n, :] = jnp.dot(onehot[0:n, :], rows, preferred_element_type=F32).astype(BF16)

    loads[0].wait()
    qt[0] = slot_table(ids_v[...])

    loads[2].wait()

    def norm(i, carry):
        rows = pl.ds(pl.multiple_of(i * 32, 32), 32)
        full = tok_v[rows, :].astype(F32)
        scale = lax.rsqrt(jnp.mean(full * full, axis=1, keepdims=True) + norm_eps)
        mine = tok_v[rows, pl.ds(pl.multiple_of(tp * COLS, COLS), COLS)].astype(F32)
        normed[rows, :] = (mine * scale).astype(BF16)
        return carry

    lax.fori_loop(0, ROWS // 32, norm, 0)

    pl.semaphore_wait(barrier, ZS * YS - 1 + 3)

    up, below = peer(1, 0), peer(2, 0)
    for side, device in enumerate((up, below)):
        remote(normed, rows_in.at[side], near_send.at[0], near_recv.at[side], device).start()
        remote(ids_v, ids_in.at[side], near_send.at[1], near_recv.at[2 + side], device).start()

    here = [plane_fs[0] + row[d] for d in range(YS)]
    slots_own = slots.at[0]
    fill(0, normed[...], here, slots_own)

    loads[3].wait()
    square = (OWN, OWN)
    gain = jnp.sum(
        jnp.where(
            lax.broadcasted_iota(jnp.int32, square, 0) == lax.broadcasted_iota(jnp.int32, square, 1),
            jnp.broadcast_to(gain_v[...], square), 0.0,
        ),
        axis=1, keepdims=True,
    )
    for i in (4, 5, 6):
        loads[i].wait()

    def fold(e, carry):
        gate, up = (gain * gate_v[e]).astype(BF16), (gain * up_v[e]).astype(BF16)
        wb1a[e, :, 0:SIDE] = gate[:, :SIDE]
        wb1a[e, :, SIDE:COLS] = up[:, :SIDE]
        wb1b[e, :, 0:SIDE] = gate[:, SIDE:]
        wb1b[e, :, SIDE:COLS] = up[:, SIDE:]
        wb2[e] = down_v[e].astype(BF16)
        return carry

    lax.fori_loop(0, EXPERTS, fold, 0)
    own_rows = pl.ds(pl.multiple_of(me * OWN, OWN), OWN)
    rcv1a[own_rows, :] = wb1a[fs]
    rcv1b[own_rows, :] = wb1b[fs]
    rcv2[own_rows, :] = wb2[fs]

    def slot_rows(e):
        return pl.ds(pl.multiple_of(e * CAP, 16), CAP)

    self_slot = 3 * 4 + y
    ag1[tp, slot_rows(self_slot), :] = slots_own[0:CAP, :]

    def routes(group):
        if group == 3:
            return [(0, d) for d in range(1, YS)]
        if group == 0:
            return [(3 + d % 2, d) for d in range(YS)]
        return [(group, d) for d in range(YS)]

    def send_slots(side, i, group, k, d):
        remote(
            slots.at[side, pl.ds(i * CAP, CAP)], ag1.at[tp, slot_rows(group * 4 + y)],
            tok_send, tok_recv.at[group], peer(k, d),
        ).start()

    for d in range(1, YS):
        send_slots(0, d, 3, 0, d)

    def send_weights(source, landing, columns, send, recv, order):
        for k, d in order:
            remote(
                source.at[plane_fs[k] + row[d], :, columns], landing.at[own_rows, columns],
                send, recv(k), peer(k, d),
            ).start()

    whole, low, high = pl.ds(0, COLS), pl.ds(0, SIDE), pl.ds(SIDE, SIDE)
    send_weights(wb1a, rcv1a, whole, w_send.at[0], lambda k: w_recv.at[0], ORDER[:AHEAD])

    loads[1].wait()
    ids, exponent = ids_v[...], jnp.exp(sc_v[...])
    total = jnp.sum(exponent, axis=0, keepdims=True)
    weights = (exponent / total).astype(BF16).astype(F32)
    weight_of = jnp.zeros((EXPERTS, ROWS), F32)
    for k in range(TOP):
        weight_of = weight_of + jnp.where(ids[k : k + 1, :] == expert_of, weights[k : k + 1, :], 0.0)
    wt[...] = weight_of

    def combine(e, carry):
        hit = qt[0, pl.ds(e, 1), :] == slot_no
        rows = pl.ds(pl.multiple_of(e * CAP, 16), CAP)
        combine_t[rows, :] = jnp.where(hit, wt[pl.ds(e, 1), :], 0.0).astype(BF16)
        return carry

    lax.fori_loop(0, EXPERTS, combine, 0)

    for side in range(2):
        landed(ids_in.at[side], near_recv.at[2 + side])
        landed(rows_in.at[side], near_recv.at[side])
        qt[1 + side] = slot_table(ids_in[side])
        beyond = [(1 + side, d) for d in range(side, YS, 2)]
        experts = here + [plane_fs[k] + row[d] for k, d in beyond]
        fill(1 + side, rows_in[side], experts, slots.at[1 + side])
        for i, (k, d) in enumerate(beyond):
            send_slots(1 + side, YS + i, 0, k, d)
        for d in range(1, YS):
            send_slots(1 + side, d, 1 + side, 0, d)
        ag1[tp, slot_rows((1 + side) * 4 + y), :] = slots[1 + side, 0:CAP, :]

    send_weights(wb1a, rcv1a, whole, w_send.at[0], lambda k: w_recv.at[0], ORDER[AHEAD:])
    send_weights(wb1b, rcv1b, whole, w_send.at[1], lambda k: w_recv.at[1], ORDER)
    send_weights(wb2, rcv2, low, w_send.at[2], lambda k: w_recv.at[2], ORDER)
    send_weights(wb2, rcv2, high, w_send.at[3], lambda k: w_recv.at[3 if k in FIRST else 4], LAST_ORDER)

    def gather(buf, columns, send, recv, sib_recv):
        def piece(xx, cc, start, size):
            return buf.at[xx * 2 + cc, pl.ds(start, size), columns]

        def own(q):
            mine = piece(x, core, q * CHUNK, CHUNK)
            remote(mine, mine, send, recv.at[0, q], right).start()
            remote(mine, mine, send, recv.at[1, q], left).start()
            remote(mine, mine, send, sib_recv, sib).start()

        def forward(q):
            whole = piece(x_left, core, q * CHUNK, CHUNK)
            landed(whole, recv.at[0, q])
            first = piece(x_left, core, q * CHUNK, HALF)
            remote(first, first, send, recv.at[2, q], right).start()
            remote(whole, whole, send, sib_recv, sib).start()
            whole = piece(x_right, core, q * CHUNK, CHUNK)
            landed(whole, recv.at[1, q])
            second = piece(x_right, core, q * CHUNK + HALF, HALF)
            remote(second, second, send, recv.at[2, q], left).start()
            remote(whole, whole, send, sib_recv, sib).start()

        def far(q):
            both = piece(x_far, core, q * CHUNK, CHUNK)
            landed(both, recv.at[2, q])
            remote(both, both, send, sib_recv, sib).start()

        def run(order, prepare):
            for i in range(CHUNKS + 3):
                if i < CHUNKS:
                    prepare(order[i])
                    own(order[i])
                if 0 <= i - 2 < CHUNKS:
                    forward(order[i - 2])
                if 0 <= i - 4:
                    far(order[i - 4])
            far(order[CHUNKS - 1])
            landed(buf.at[pl.ds(0, 4), :, columns], sib_recv)

        return run

    def group_landed(q):
        landed(ag1.at[0, pl.ds(0, (4 if q == 0 else 3) * CAP)], tok_recv.at[q])

    gather(ag1, whole, ag_send.at[0], ag1_recv, sib_recv.at[0])((3, 1, 2, 0), group_landed)

    def product(left_of, right_of, rows, columns, ks):
        total = None
        for k in ks:
            j = planes[k] if isinstance(ks, tuple) else k
            start = pl.multiple_of(j * COLS, COLS) if isinstance(ks, tuple) else k * COLS
            part = jnp.dot(
                left_of[j, rows, :], right_of[pl.ds(start, COLS), columns],
                preferred_element_type=F32,
            )
            total = part if total is None else total + part
        return total

    def half(landing, side, columns, hidden_recv):
        def hidden(q):
            rows = pl.ds(q * CHUNK, CHUNK)
            pre = product(ag1, landing, rows, whole, range(ZS))
            g = jnp.minimum(pre[:, :SIDE], clamp_limit)
            v = jnp.clip(pre[:, SIDE:], -clamp_limit, clamp_limit)
            ag2[tp, rows, columns] = (g * jax.nn.sigmoid(sigmoid_slope * g) * (v + 1.0)).astype(BF16)

        landed(landing.at[pl.ds(0, 31 * OWN)], w_recv.at[side])
        gather(ag2, columns, ag_send.at[1 + side], hidden_recv, sib_recv.at[1 + side])(
            tuple(range(CHUNKS)), hidden
        )

    half(rcv1a, 0, low, ag2a_recv)
    half(rcv1b, 1, high, ag2b_recv)

    def back(group, side, columns):
        for k, d in routes(group):
            away = (0, 2, 1, 4, 3)[k]
            remote(
                res.at[slot_rows(group * 4 + row[d]), columns], ret.at[slot_rows(fs), columns],
                ret_send.at[side], ret_recv.at[side], peer(away, d),
            ).start()

    landed(rcv2.at[pl.ds(0, 31 * OWN), low], w_recv.at[2])
    for r in range(CHUNKS):
        rows = pl.ds(r * CHUNK, CHUNK)
        res[rows, low] = product(ag2, rcv2, rows, low, range(ZS)).astype(BF16)
        back(r, 0, low)

    landed(rcv2.at[pl.ds(0, (4 * len(FIRST) - (0 in FIRST)) * OWN), high], w_recv.at[3])

    def begin(r, carry):
        rows = pl.ds(pl.multiple_of(r * CHUNK, CHUNK), CHUNK)
        acc[rows, :] = product(ag2, rcv2, rows, high, tuple(FIRST))
        return carry

    lax.fori_loop(0, CHUNKS, begin, 0)
    landed(rcv2.at[pl.ds(0, (4 * len(LATER) - (0 in LATER)) * OWN), high], w_recv.at[4])
    for r in range(CHUNKS):
        rows = pl.ds(r * CHUNK, CHUNK)
        late = product(ag2, rcv2, rows, high, tuple(LATER))
        res[rows, high] = (acc[rows, :] + late).astype(BF16)
        back(r, 1, high)
    ret[slot_rows(fs), :] = res[slot_rows(self_slot), :]

    landed(ret.at[pl.ds(0, 13 * CAP)], tok_send)
    landed(rows_in, near_send.at[0])
    landed(ids_in, near_send.at[1])
    for i, landing in enumerate((rcv1a, rcv1b, rcv2.at[:, low], rcv2.at[:, high])):
        landed(landing.at[pl.ds(0, 31 * OWN)], w_send.at[i])
    landed(ag1.at[pl.ds(0, 7)], ag_send.at[0])
    for side in range(2):
        landed(ag2.at[pl.ds(0, 7), :, pl.ds(0, SIDE)], ag_send.at[1 + side])
        landed(ret.at[pl.ds(0, SLOTS - CAP), pl.ds(0, SIDE)], ret_send.at[side])
    for side in range(2):
        landed(ret.at[pl.ds(0, SLOTS - CAP), pl.ds(side * SIDE, SIDE)], ret_recv.at[side])


def write_out(rcv1a, rcv1b, rcv2, ret, combine_t, og, ou, od, om, mix_v, sem):
    low, high = pl.ds(0, SIDE), pl.ds(SIDE, SIDE)
    copies = [
        pltpu.make_async_copy(s, d, sem.at[i])
        for i, (s, d) in enumerate((
            (rcv1a.at[:, low], og.at[0, :, low]), (rcv1b.at[:, low], og.at[0, :, high]),
            (rcv1a.at[:, high], ou.at[0, :, low]), (rcv1b.at[:, high], ou.at[0, :, high]),
            (rcv2, od.at[0]),
        ))
    ]
    for c in copies:
        c.start()
    mix_v[...] = lax.dot_general(
        combine_t[...], ret[...], (((0,), (0,)), ((), ())), preferred_element_type=F32
    ).astype(BF16)
    mix_out = pltpu.make_async_copy(mix_v, om, sem.at[5])
    mix_out.start()
    for c in copies:
        c.wait()
    mix_out.wait()


def local(tokens, route_ids, route_scores, norm_gain, gate_weight, up_weight, down_weight):
    hbm, vmem = pl.BlockSpec(memory_space=pltpu.HBM), pl.BlockSpec(memory_space=pltpu.VMEM)
    dma = pltpu.SemaphoreType.DMA
    rows = jax.ShapeDtypeStruct((2048, COLS), BF16)
    slots = jax.ShapeDtypeStruct((SLOTS, COLS), BF16)
    landed = pl.pallas_call(
        kernel,
        name="hand_over",
        out_shape=(rows, rows, rows, slots, slots),
        in_specs=[hbm] * 7,
        out_specs=[vmem] * 5,
        scratch_shapes=[
            pltpu.VMEM((ROWS, 2048), BF16),
            pltpu.VMEM((TOP, ROWS), jnp.int32),
            pltpu.VMEM((TOP, ROWS), F32),
            pltpu.VMEM((1, OWN), F32),
            pltpu.VMEM((EXPERTS, OWN, COLS), F32),
            pltpu.VMEM((EXPERTS, OWN, COLS), F32),
            pltpu.VMEM((EXPERTS, OWN, COLS), F32),
            pltpu.VMEM((3, EXPERTS, ROWS), F32),
            pltpu.VMEM((EXPERTS, ROWS), F32),
            pltpu.VMEM((6 * CAP, ROWS), BF16),
            pltpu.VMEM((ROWS, COLS), BF16),
            pltpu.VMEM((3, 6 * CAP, COLS), BF16),
            pltpu.VMEM((2, ROWS, COLS), BF16),
            pltpu.VMEM((2, TOP, ROWS), jnp.int32),
            pltpu.VMEM((EXPERTS, OWN, COLS), BF16),
            pltpu.VMEM((EXPERTS, OWN, COLS), BF16),
            pltpu.VMEM((EXPERTS, OWN, COLS), BF16),
            pltpu.VMEM((TPS, SLOTS, COLS), BF16),
            pltpu.VMEM((TPS, SLOTS, COLS), BF16),
            pltpu.VMEM((SLOTS, SIDE), F32),
            pltpu.VMEM((SLOTS, COLS), BF16),
            dma((7,)), dma((2,)), dma((4,)), dma(()), dma((4,)), dma((4,)), dma((5,)),
            dma((3,)), dma((3, CHUNKS)), dma((3, CHUNKS)), dma((3, CHUNKS)), dma((3,)),
            dma((2,)), dma((2,)),
        ],
        compiler_params=pltpu.CompilerParams(
            collective_id=0, has_side_effects=True, vmem_limit_bytes=44 * 1024 * 1024
        ),
    )(
        *(
            pltpu.with_memory_space_constraint(a, pltpu.HBM)
            for a in (tokens, route_ids.T, route_scores.T, norm_gain.reshape(1, OWN),
                      gate_weight, up_weight, down_weight)
        )
    )
    served = jax.ShapeDtypeStruct((1, 2048, COLS), BF16)
    return pl.pallas_call(
        write_out,
        name="write_out",
        out_shape=(served, served, served, jax.ShapeDtypeStruct((ROWS, COLS), BF16)),
        in_specs=[vmem] * 5,
        out_specs=[hbm] * 4,
        scratch_shapes=[pltpu.VMEM((ROWS, COLS), BF16), dma((6,))],
        compiler_params=pltpu.CompilerParams(vmem_limit_bytes=12 * 1024 * 1024),
    )(*landed)


def solution(mesh):
    in_specs = (
        P(("gr", "fs"), None),
        P(("gr", "fs"), None),
        P(("gr", "fs"), None),
        P(("gr", "fs")),
        P(None, ("gr", "fs"), "tp"),
        P(None, ("gr", "fs"), "tp"),
        P(None, ("gr", "fs"), "tp"),
    )
    out_specs = (
        P("fs", None, "tp"),
        P("fs", None, "tp"),
        P("fs", None, "tp"),
        P(("gr", "fs"), "tp"),
    )
    return jax.shard_map(local, mesh=mesh, in_specs=in_specs, out_specs=out_specs, check_vma=False)
```

```python
import jax
import jax.numpy as jnp
from jax import lax
from jax.experimental import pallas as pl
from jax.experimental.pallas import tpu as pltpu
from jax.sharding import PartitionSpec as P

MESH = pl.DeviceIdType.MESH
BF16, F32 = jnp.bfloat16, jnp.float32

EXPERTS = 16
TOP = 4
CAP = 80
ROWS = 256
SLOTS = EXPERTS * CAP
COLS = 256
SIDE = COLS // 2
TPS = 8
ZS, YS, XS = 8, 4, 4
OWN = 64
CHUNKS = 4
CHUNK = SLOTS // CHUNKS
HALF = CHUNK // 2
AHEAD = 6

norm_eps = 1e-06
clamp_limit = 7.0
sigmoid_slope = 1.702


SEQ = [7, 5, 6, 3, 4, 1, 2, 0]
FIRST, LATER = [0, 7, 5, 6, 3, 4], [1, 2]
ORDER = [(k, d) for d in (2, 1, 3, 0) for k in SEQ if k or d]
LAST_ORDER = [(k, d) for k in FIRST + LATER for d in (2, 1, 3, 0) if k or d]


def rem(a, n):
    return lax.rem(a, n)


def kernel(
    tok_h, ids_h, sc_h, gain_h, gate_h, up_h, down_h,
    rcv1a, rcv1b, rcv2, ret, combine_t,
    tok_v, ids_v, sc_v, gain_v, gate_v, up_v, down_v,
    qt, wt, onehot, normed, slots, rows_in, ids_in,
    wb1a, wb1b, wb2, ag1, ag2, acc, res,
    load_sem, near_send, near_recv, tok_send, tok_recv, w_send, w_recv,
    ag_send, ag1_recv, ag2a_recv, ag2b_recv, sib_recv, ret_send, ret_recv,
):
    gr, fs, tp = lax.axis_index("gr"), lax.axis_index("fs"), lax.axis_index("tp")
    z, y = gr * 4 + fs // 4, rem(fs, 4)
    x, core = tp // 2, rem(tp, 2)
    me = z * YS + y

    def along(xx, cc):
        return (gr, fs, xx * 2 + cc)

    x_right, x_left, x_far = rem(x + 1, XS), rem(x + 3, XS), rem(x + 2, XS)
    right, left, sib = along(x_right, core), along(x_left, core), along(x, 1 - core)

    def remote(src, dst, send, recv, device):
        return pltpu.make_async_remote_copy(
            src_ref=src, dst_ref=dst, send_sem=send, recv_sem=recv,
            device_id=device, device_id_type=MESH,
        )

    def landed(ref, sem):
        pltpu.make_async_copy(ref, ref, sem).wait()

    planes = [rem(z + (away % ZS), ZS) for away in (0, 1, -1, 2, -2, 3, -3, 4)]
    plane_gr, plane_fs = [p // 4 for p in planes], [rem(p, 4) * 4 for p in planes]
    row = [y] + [rem(y + d, YS) for d in range(1, YS)]
    peers = [(k, d) for k in range(ZS) for d in range(YS)][1:]

    def peer(k, d):
        return (plane_gr[k], plane_fs[k] + row[d], tp)

    barrier = pltpu.get_barrier_semaphore()
    for k, d in peers[::-1]:
        pl.semaphore_signal(barrier, inc=1, device_id=peer(k, d), device_id_type=MESH)
    for d in (right, left, sib):
        pl.semaphore_signal(barrier, inc=1, device_id=d, device_id_type=MESH)

    loads = [
        pltpu.make_async_copy(s, d, load_sem.at[i])
        for i, (s, d) in enumerate(
            ((ids_h, ids_v), (sc_h, sc_v), (tok_h, tok_v), (gain_h, gain_v),
             (gate_h, gate_v), (up_h, up_v), (down_h, down_v))
        )
    ]
    for c in loads:
        c.start()

    expert_of = lax.broadcasted_iota(jnp.int32, (EXPERTS, ROWS), 0)
    earlier = jnp.where(
        lax.broadcasted_iota(jnp.int32, (ROWS, ROWS), 0)
        < lax.broadcasted_iota(jnp.int32, (ROWS, ROWS), 1),
        1.0, 0.0,
    ).astype(BF16)

    def slot_table(ids):
        member = jnp.zeros((EXPERTS, ROWS), F32)
        for k in range(TOP):
            member = member + jnp.where(ids[k : k + 1, :] == expert_of, 1.0, 0.0)
        before = jnp.dot(member.astype(BF16), earlier, preferred_element_type=F32)
        return jnp.where(member > 0.5, before, -1.0)

    slot_no = lax.broadcasted_iota(jnp.int32, (CAP, ROWS), 0).astype(F32)

    def fill(table, rows, experts, out):
        for i, e in enumerate(experts):
            hit = qt[table, pl.ds(e, 1), :] == slot_no
            onehot[i * CAP : (i + 1) * CAP, :] = jnp.where(hit, 1.0, 0.0).astype(BF16)
        n = len(experts) * CAP
        out[0:n, :] = jnp.dot(onehot[0:n, :], rows, preferred_element_type=F32).astype(BF16)

    loads[0].wait()
    qt[0] = slot_table(ids_v[...])

    loads[2].wait()

    def norm(i, carry):
        rows = pl.ds(pl.multiple_of(i * 32, 32), 32)
        full = tok_v[rows, :].astype(F32)
        scale = lax.rsqrt(jnp.mean(full * full, axis=1, keepdims=True) + norm_eps)
        mine = tok_v[rows, pl.ds(pl.multiple_of(tp * COLS, COLS), COLS)].astype(F32)
        normed[rows, :] = (mine * scale).astype(BF16)
        return carry

    lax.fori_loop(0, ROWS // 32, norm, 0)

    pl.semaphore_wait(barrier, ZS * YS - 1 + 3)

    up, below = peer(1, 0), peer(2, 0)
    for side, device in enumerate((up, below)):
        remote(normed, rows_in.at[side], near_send.at[0], near_recv.at[side], device).start()
        remote(ids_v, ids_in.at[side], near_send.at[1], near_recv.at[2 + side], device).start()

    here = [plane_fs[0] + row[d] for d in range(YS)]
    slots_own = slots.at[0]
    fill(0, normed[...], here, slots_own)

    loads[3].wait()
    square = (OWN, OWN)
    gain = jnp.sum(
        jnp.where(
            lax.broadcasted_iota(jnp.int32, square, 0) == lax.broadcasted_iota(jnp.int32, square, 1),
            jnp.broadcast_to(gain_v[...], square), 0.0,
        ),
        axis=1, keepdims=True,
    )
    for i in (4, 5, 6):
        loads[i].wait()

    def fold(e, carry):
        gate, up = (gain * gate_v[e]).astype(BF16), (gain * up_v[e]).astype(BF16)
        wb1a[e, :, 0:SIDE] = gate[:, :SIDE]
        wb1a[e, :, SIDE:COLS] = up[:, :SIDE]
        wb1b[e, :, 0:SIDE] = gate[:, SIDE:]
        wb1b[e, :, SIDE:COLS] = up[:, SIDE:]
        wb2[e] = down_v[e].astype(BF16)
        return carry

    lax.fori_loop(0, EXPERTS, fold, 0)
    own_rows = pl.ds(pl.multiple_of(me * OWN, OWN), OWN)
    rcv1a[own_rows, :] = wb1a[fs]
    rcv1b[own_rows, :] = wb1b[fs]
    rcv2[own_rows, :] = wb2[fs]

    def slot_rows(e):
        return pl.ds(pl.multiple_of(e * CAP, 16), CAP)

    self_slot = 3 * 4 + y
    ag1[tp, slot_rows(self_slot), :] = slots_own[0:CAP, :]

    def routes(group):
        if group == 3:
            return [(0, d) for d in range(1, YS)]
        if group == 0:
            return [(3 + d % 2, d) for d in range(YS)]
        return [(group, d) for d in range(YS)]

    def send_slots(side, i, group, k, d):
        remote(
            slots.at[side, pl.ds(i * CAP, CAP)], ag1.at[tp, slot_rows(group * 4 + y)],
            tok_send, tok_recv.at[group], peer(k, d),
        ).start()

    for d in range(1, YS):
        send_slots(0, d, 3, 0, d)

    def send_weights(source, landing, columns, send, recv, order):
        for k, d in order:
            remote(
                source.at[plane_fs[k] + row[d], :, columns], landing.at[own_rows, columns],
                send, recv(k), peer(k, d),
            ).start()

    whole, low, high = pl.ds(0, COLS), pl.ds(0, SIDE), pl.ds(SIDE, SIDE)
    send_weights(wb1a, rcv1a, whole, w_send.at[0], lambda k: w_recv.at[0], ORDER[:AHEAD])

    loads[1].wait()
    ids, exponent = ids_v[...], jnp.exp(sc_v[...])
    total = jnp.sum(exponent, axis=0, keepdims=True)
    weights = (exponent / total).astype(BF16).astype(F32)
    weight_of = jnp.zeros((EXPERTS, ROWS), F32)
    for k in range(TOP):
        weight_of = weight_of + jnp.where(ids[k : k + 1, :] == expert_of, weights[k : k + 1, :], 0.0)
    wt[...] = weight_of

    def combine(e, carry):
        hit = qt[0, pl.ds(e, 1), :] == slot_no
        rows = pl.ds(pl.multiple_of(e * CAP, 16), CAP)
        combine_t[rows, :] = jnp.where(hit, wt[pl.ds(e, 1), :], 0.0).astype(BF16)
        return carry

    lax.fori_loop(0, EXPERTS, combine, 0)

    for side in range(2):
        landed(ids_in.at[side], near_recv.at[2 + side])
        landed(rows_in.at[side], near_recv.at[side])
        qt[1 + side] = slot_table(ids_in[side])
        beyond = [(1 + side, d) for d in range(side, YS, 2)]
        experts = here + [plane_fs[k] + row[d] for k, d in beyond]
        fill(1 + side, rows_in[side], experts, slots.at[1 + side])
        for i, (k, d) in enumerate(beyond):
            send_slots(1 + side, YS + i, 0, k, d)
        for d in range(1, YS):
            send_slots(1 + side, d, 1 + side, 0, d)
        ag1[tp, slot_rows((1 + side) * 4 + y), :] = slots[1 + side, 0:CAP, :]

    send_weights(wb1a, rcv1a, whole, w_send.at[0], lambda k: w_recv.at[0], ORDER[AHEAD:])
    send_weights(wb1b, rcv1b, whole, w_send.at[1], lambda k: w_recv.at[1], ORDER)
    send_weights(wb2, rcv2, low, w_send.at[2], lambda k: w_recv.at[2], ORDER)
    send_weights(wb2, rcv2, high, w_send.at[3], lambda k: w_recv.at[3 if k in FIRST else 4], LAST_ORDER)

    def gather(buf, columns, send, recv, sib_recv):
        def piece(xx, cc, start, size):
            return buf.at[xx * 2 + cc, pl.ds(start, size), columns]

        def own(q):
            mine = piece(x, core, q * CHUNK, CHUNK)
            remote(mine, mine, send, recv.at[0, q], right).start()
            remote(mine, mine, send, recv.at[1, q], left).start()
            remote(mine, mine, send, sib_recv, sib).start()

        def forward(q):
            whole = piece(x_left, core, q * CHUNK, CHUNK)
            landed(whole, recv.at[0, q])
            first = piece(x_left, core, q * CHUNK, HALF)
            remote(first, first, send, recv.at[2, q], right).start()
            remote(whole, whole, send, sib_recv, sib).start()
            whole = piece(x_right, core, q * CHUNK, CHUNK)
            landed(whole, recv.at[1, q])
            second = piece(x_right, core, q * CHUNK + HALF, HALF)
            remote(second, second, send, recv.at[2, q], left).start()
            remote(whole, whole, send, sib_recv, sib).start()

        def far(q):
            both = piece(x_far, core, q * CHUNK, CHUNK)
            landed(both, recv.at[2, q])
            remote(both, both, send, sib_recv, sib).start()

        def run(order, prepare):
            for i in range(CHUNKS + 3):
                if i < CHUNKS:
                    prepare(order[i])
                    own(order[i])
                if 0 <= i - 2 < CHUNKS:
                    forward(order[i - 2])
                if 0 <= i - 4:
                    far(order[i - 4])
            far(order[CHUNKS - 1])
            landed(buf.at[pl.ds(0, 4), :, columns], sib_recv)

        return run

    def group_landed(q):
        landed(ag1.at[0, pl.ds(0, (4 if q == 0 else 3) * CAP)], tok_recv.at[q])

    gather(ag1, whole, ag_send.at[0], ag1_recv, sib_recv.at[0])((3, 1, 2, 0), group_landed)

    def product(left_of, right_of, rows, columns, ks):
        total = None
        for k in ks:
            j = planes[k] if isinstance(ks, tuple) else k
            start = pl.multiple_of(j * COLS, COLS) if isinstance(ks, tuple) else k * COLS
            part = jnp.dot(
                left_of[j, rows, :], right_of[pl.ds(start, COLS), columns],
                preferred_element_type=F32,
            )
            total = part if total is None else total + part
        return total

    def half(landing, side, columns, hidden_recv):
        def hidden(q):
            rows = pl.ds(q * CHUNK, CHUNK)
            pre = product(ag1, landing, rows, whole, range(ZS))
            g = jnp.minimum(pre[:, :SIDE], clamp_limit)
            v = jnp.clip(pre[:, SIDE:], -clamp_limit, clamp_limit)
            ag2[tp, rows, columns] = (g * jax.nn.sigmoid(sigmoid_slope * g) * (v + 1.0)).astype(BF16)

        landed(landing.at[pl.ds(0, 31 * OWN)], w_recv.at[side])
        gather(ag2, columns, ag_send.at[1 + side], hidden_recv, sib_recv.at[1 + side])(
            tuple(range(CHUNKS)), hidden
        )

    half(rcv1a, 0, low, ag2a_recv)
    half(rcv1b, 1, high, ag2b_recv)

    def back(group, side, columns):
        for k, d in routes(group):
            away = (0, 2, 1, 4, 3)[k]
            remote(
                res.at[slot_rows(group * 4 + row[d]), columns], ret.at[slot_rows(fs), columns],
                ret_send.at[side], ret_recv.at[side], peer(away, d),
            ).start()

    landed(rcv2.at[pl.ds(0, 31 * OWN), low], w_recv.at[2])
    for r in range(CHUNKS):
        rows = pl.ds(r * CHUNK, CHUNK)
        res[rows, low] = product(ag2, rcv2, rows, low, range(ZS)).astype(BF16)
        back(r, 0, low)

    landed(rcv2.at[pl.ds(0, (4 * len(FIRST) - (0 in FIRST)) * OWN), high], w_recv.at[3])

    def begin(r, carry):
        rows = pl.ds(pl.multiple_of(r * CHUNK, CHUNK), CHUNK)
        acc[rows, :] = product(ag2, rcv2, rows, high, tuple(FIRST))
        return carry

    lax.fori_loop(0, CHUNKS, begin, 0)
    landed(rcv2.at[pl.ds(0, (4 * len(LATER) - (0 in LATER)) * OWN), high], w_recv.at[4])
    for r in range(CHUNKS):
        rows = pl.ds(r * CHUNK, CHUNK)
        late = product(ag2, rcv2, rows, high, tuple(LATER))
        res[rows, high] = (acc[rows, :] + late).astype(BF16)
        back(r, 1, high)
    ret[slot_rows(fs), :] = res[slot_rows(self_slot), :]

    landed(ret.at[pl.ds(0, 13 * CAP)], tok_send)
    landed(rows_in, near_send.at[0])
    landed(ids_in, near_send.at[1])
    for i, landing in enumerate((rcv1a, rcv1b, rcv2.at[:, low], rcv2.at[:, high])):
        landed(landing.at[pl.ds(0, 31 * OWN)], w_send.at[i])
    landed(ag1.at[pl.ds(0, 7)], ag_send.at[0])
    for side in range(2):
        landed(ag2.at[pl.ds(0, 7), :, pl.ds(0, SIDE)], ag_send.at[1 + side])
        landed(ret.at[pl.ds(0, SLOTS - CAP), pl.ds(0, SIDE)], ret_send.at[side])
    for side in range(2):
        landed(ret.at[pl.ds(0, SLOTS - CAP), pl.ds(side * SIDE, SIDE)], ret_recv.at[side])


def write_out(rcv1a, rcv1b, rcv2, ret, combine_t, og, ou, od, om, mix_v, sem):
    low, high = pl.ds(0, SIDE), pl.ds(SIDE, SIDE)
    copies = [
        pltpu.make_async_copy(s, d, sem.at[i])
        for i, (s, d) in enumerate((
            (rcv1a.at[:, low], og.at[0, :, low]), (rcv1b.at[:, low], og.at[0, :, high]),
            (rcv1a.at[:, high], ou.at[0, :, low]), (rcv1b.at[:, high], ou.at[0, :, high]),
            (rcv2, od.at[0]),
        ))
    ]
    for c in copies:
        c.start()
    mix_v[...] = lax.dot_general(
        combine_t[...], ret[...], (((0,), (0,)), ((), ())), preferred_element_type=F32
    ).astype(BF16)
    mix_out = pltpu.make_async_copy(mix_v, om, sem.at[5])
    mix_out.start()
    for c in copies:
        c.wait()
    mix_out.wait()


def local(tokens, route_ids, route_scores, norm_gain, gate_weight, up_weight, down_weight):
    hbm, vmem = pl.BlockSpec(memory_space=pltpu.HBM), pl.BlockSpec(memory_space=pltpu.VMEM)
    dma = pltpu.SemaphoreType.DMA
    rows = jax.ShapeDtypeStruct((2048, COLS), BF16)
    slots = jax.ShapeDtypeStruct((SLOTS, COLS), BF16)
    landed = pl.pallas_call(
        kernel,
        name="hand_over",
        out_shape=(rows, rows, rows, slots, slots),
        in_specs=[hbm] * 7,
        out_specs=[vmem] * 5,
        scratch_shapes=[
            pltpu.VMEM((ROWS, 2048), BF16),
            pltpu.VMEM((TOP, ROWS), jnp.int32),
            pltpu.VMEM((TOP, ROWS), F32),
            pltpu.VMEM((1, OWN), F32),
            pltpu.VMEM((EXPERTS, OWN, COLS), F32),
            pltpu.VMEM((EXPERTS, OWN, COLS), F32),
            pltpu.VMEM((EXPERTS, OWN, COLS), F32),
            pltpu.VMEM((3, EXPERTS, ROWS), F32),
            pltpu.VMEM((EXPERTS, ROWS), F32),
            pltpu.VMEM((6 * CAP, ROWS), BF16),
            pltpu.VMEM((ROWS, COLS), BF16),
            pltpu.VMEM((3, 6 * CAP, COLS), BF16),
            pltpu.VMEM((2, ROWS, COLS), BF16),
            pltpu.VMEM((2, TOP, ROWS), jnp.int32),
            pltpu.VMEM((EXPERTS, OWN, COLS), BF16),
            pltpu.VMEM((EXPERTS, OWN, COLS), BF16),
            pltpu.VMEM((EXPERTS, OWN, COLS), BF16),
            pltpu.VMEM((TPS, SLOTS, COLS), BF16),
            pltpu.VMEM((TPS, SLOTS, COLS), BF16),
            pltpu.VMEM((SLOTS, SIDE), F32),
            pltpu.VMEM((SLOTS, COLS), BF16),
            dma((7,)), dma((2,)), dma((4,)), dma(()), dma((4,)), dma((4,)), dma((5,)),
            dma((3,)), dma((3, CHUNKS)), dma((3, CHUNKS)), dma((3, CHUNKS)), dma((3,)),
            dma((2,)), dma((2,)),
        ],
        compiler_params=pltpu.CompilerParams(
            collective_id=0, has_side_effects=True, vmem_limit_bytes=44 * 1024 * 1024
        ),
    )(
        *(
            pltpu.with_memory_space_constraint(a, pltpu.HBM)
            for a in (tokens, route_ids.T, route_scores.T, norm_gain.reshape(1, OWN),
                      gate_weight, up_weight, down_weight)
        )
    )
    served = jax.ShapeDtypeStruct((1, 2048, COLS), BF16)
    return pl.pallas_call(
        write_out,
        name="write_out",
        out_shape=(served, served, served, jax.ShapeDtypeStruct((ROWS, COLS), BF16)),
        in_specs=[vmem] * 5,
        out_specs=[hbm] * 4,
        scratch_shapes=[pltpu.VMEM((ROWS, COLS), BF16), dma((6,))],
        compiler_params=pltpu.CompilerParams(vmem_limit_bytes=12 * 1024 * 1024),
    )(*landed)


def solution(mesh):
    in_specs = (
        P(("gr", "fs"), None),
        P(("gr", "fs"), None),
        P(("gr", "fs"), None),
        P(("gr", "fs")),
        P(None, ("gr", "fs"), "tp"),
        P(None, ("gr", "fs"), "tp"),
        P(None, ("gr", "fs"), "tp"),
    )
    out_specs = (
        P("fs", None, "tp"),
        P("fs", None, "tp"),
        P("fs", None, "tp"),
        P(("gr", "fs"), "tp"),
    )
    return jax.shard_map(local, mesh=mesh, in_specs=in_specs, out_specs=out_specs, check_vma=False)
```
